256 devices in a mesh: kv: 16 (over y, x), tp: 16 (over z, core).
Axes of the slice: x: 4, y: 4, z: 8, core: 2. Of those that a mesh axis runs over, the one named last changes fastest.
Arguments:
- tokens: bfloat16 [640, 4096], P('tp', 'kv'), may hold values from -8 to 8
- state: float32 [640, 32, 128, 128], P('kv', 'tp'), may hold values from -4 to 4
- mix_gain: float32 [4096], P('kv'), may hold values from 0.1 to 1.9
- q_weight: bfloat16 [4096, 4096], P('kv', 'tp'), may hold values from -0.09375 to 0.09375
- forget_weight: bfloat16 [4096, 4096], P('kv', 'tp'), may hold values from -0.09375 to 0.09375
- input_weight: bfloat16 [4096, 4096], P('kv', 'tp'), may hold values from -0.09375 to 0.09375
- gate_weight: bfloat16 [4096, 4096], P('kv', 'tp'), may hold values from -0.09375 to 0.09375
- lower_bound: float32 [4096], P('tp'), may hold values from 0 to 0.9
- head_gain: float32 [128], replicated, may hold values from 0.1 to 1.9
- out_weight: bfloat16 [4096, 4096], P('tp', 'kv'), may hold values from -0.09375 to 0.09375
- ffn_gain: float32 [4096], P('kv'), may hold values from 0.1 to 1.9
- ffn_gate: bfloat16 [4096, 10240], P('kv', 'tp'), may hold values from -0.09375 to 0.09375
- ffn_up: bfloat16 [4096, 10240], P('kv', 'tp'), may hold values from -0.09375 to 0.09375
- ffn_down: bfloat16 [10240, 4096], P('tp', 'kv'), may hold values from -0.0625 to 0.0625
Outputs:
- layer_out: bfloat16 [640, 4096], P('tp', 'kv')
- new_state: float32 [640, 32, 128, 128], P('kv', 'tp')
The draws below stay inside these ranges and needn't reach their ends.
All inputs are finite; a program needn't handle non-finite values.
Results may differ from the reference program's by a relative error of at most 0.007.
Values may be sent and summed in bfloat16 or wider, within the bound.
A program may use at most 64 MiB of HBM per device.

```python
import jax
import jax.numpy as jnp
from jax import lax

HEADS = 32
HEAD = 128
D = 4096
FF = 10240
BATCH = 640


def draw_tokens(key, part):
    first, second, third, fourth = jax.random.split(jax.random.fold_in(key, 17), 4)
    base = jax.random.normal(first, (BATCH, D), jnp.float32)
    block_scale = jnp.exp(jax.random.uniform(second, (32,), jnp.float32, -1.2, 1.2))
    column_scale = jnp.repeat(block_scale, D // 32)
    values = base * column_scale[None, :]
    return jnp.clip(values, -8.0, 8.0).astype(jnp.bfloat16)


def levels(stream_key, shape, cuts, least, top_value):
    def one(axis_at, parts):
        draws = jax.random.uniform(jax.random.fold_in(jax.random.fold_in(stream_key, 6), axis_at), (parts,), jnp.float32, least / len(cuts), top_value / len(cuts))
        return jnp.repeat(jnp.exp(draws), shape[axis_at] // parts).reshape((-1,) + (1,) * (len(shape) - axis_at - 1))

    loudness = one(*cuts[0])
    for cut in cuts[1:]:
        loudness = loudness * one(*cut)
    return loudness


def gaussian(key, shape, scale, bound, shards=(), kind=jnp.bfloat16):
    array = scale * jax.random.normal(key, shape, jnp.float32)
    if shards:
        array = array * levels(key, shape, shards, -0.22, 0.18)
    return jnp.clip(array, -bound, bound).astype(kind)


def setup_inputs(seed: int = 0) -> dict:
    key_of = jax.random.split(jax.random.key(seed), 15)
    tokens = draw_tokens(jax.random.fold_in(key_of[14], 71), 0)
    state = gaussian(key_of[1], (BATCH, HEADS, HEAD, HEAD), 0.5, 4.0, ((0, 16), (1, 16)), jnp.float32)
    mix_gain = jnp.clip(1.0 + 0.18 * jax.random.normal(key_of[2], (D,), jnp.float32), 0.1, 1.9)
    q_weight = gaussian(key_of[3], (D, D), D ** -0.5, 0.09375, ((0, 16), (1, 16)))
    forget_weight = gaussian(key_of[4], (D, D), D ** -0.5, 0.09375, ((0, 16), (1, 16)))
    input_weight = gaussian(key_of[5], (D, D), D ** -0.5, 0.09375, ((0, 16), (1, 16)))
    gate_weight = gaussian(key_of[6], (D, D), D ** -0.5, 0.09375, ((0, 16), (1, 16)))
    lower_bound = jnp.clip(0.9 * jax.random.uniform(key_of[7], (D,), jnp.float32) ** levels(key_of[7], (D,), ((0, 16),), -0.2, 0.2), 0.0, 0.9)
    head_gain = jnp.clip(1.0 + 0.18 * jax.random.normal(key_of[8], (HEAD,), jnp.float32), 0.1, 1.9)
    out_weight = gaussian(key_of[9], (D, D), D ** -0.5, 0.09375, ((0, 16), (1, 16)))
    ffn_gain = jnp.clip(1.0 + 0.18 * jax.random.normal(key_of[10], (D,), jnp.float32), 0.1, 1.9)
    ffn_gate = gaussian(key_of[11], (D, FF), D ** -0.5, 0.09375, ((0, 16), (1, 16)))
    ffn_up = gaussian(key_of[12], (D, FF), D ** -0.5, 0.09375, ((0, 16), (1, 16)))
    ffn_down = gaussian(key_of[13], (FF, D), FF ** -0.5, 0.0625, ((0, 16), (1, 16)))
    return {"tokens": tokens, "state": state, "mix_gain": mix_gain, "q_weight": q_weight, "forget_weight": forget_weight, "input_weight": input_weight, "gate_weight": gate_weight, "lower_bound": lower_bound, "head_gain": head_gain, "out_weight": out_weight, "ffn_gain": ffn_gain, "ffn_gate": ffn_gate, "ffn_up": ffn_up, "ffn_down": ffn_down}


EPS = 1e-05

def reference(tokens, state, mix_gain, q_weight, forget_weight, input_weight, gate_weight, lower_bound, head_gain, out_weight, ffn_gain, ffn_gate, ffn_up, ffn_down):
    batch_rows = tokens.shape[0]
    values = tokens.astype(jnp.float32)
    factor = lax.rsqrt(lax.optimization_barrier(jnp.mean(values * values, axis=1, keepdims=True)) + EPS)
    normed = (values * mix_gain).astype(jnp.bfloat16)

    def project(weight):
        return jnp.dot(normed, weight, preferred_element_type=jnp.float32) * factor
    query_pre = project(q_weight)
    forget_pre = project(forget_weight)
    value_pre = project(input_weight)
    gate_pre = project(gate_weight)
    split_shape = (batch_rows, HEADS, HEAD)
    query = (jax.nn.silu(query_pre) * HEAD ** (-0.5)).reshape(split_shape)
    forget = (lower_bound + (1.0 - lower_bound) * jax.nn.sigmoid(forget_pre)).reshape(split_shape)
    value = value_pre.reshape(split_shape)
    new_state = forget[..., None] * state + (1.0 - forget)[..., None] * value[:, :, None, :]
    read = jnp.einsum('bhk,bhkv->bhv', query, new_state, precision=lax.Precision.HIGHEST)
    read = read * lax.rsqrt(lax.optimization_barrier(jnp.mean(read * read, axis=-1, keepdims=True)) + EPS) * head_gain
    gated = (read.reshape(batch_rows, D) * jax.nn.silu(gate_pre)).astype(jnp.bfloat16)
    residual = (values + jnp.dot(gated, out_weight, preferred_element_type=jnp.float32)).astype(jnp.bfloat16)
    res_values = residual.astype(jnp.float32)
    factor_ffn = lax.rsqrt(lax.optimization_barrier(jnp.mean(res_values * res_values, axis=1, keepdims=True)) + EPS)
    normed_ffn = (res_values * ffn_gain).astype(jnp.bfloat16)
    gate_ffn = jnp.dot(normed_ffn, ffn_gate, preferred_element_type=jnp.float32) * factor_ffn
    up_ffn = jnp.dot(normed_ffn, ffn_up, preferred_element_type=jnp.float32) * factor_ffn
    hidden = (jax.nn.silu(gate_ffn) * up_ffn).astype(jnp.bfloat16)
    layer_out = (res_values + jnp.dot(hidden, ffn_down, preferred_element_type=jnp.float32)).astype(jnp.bfloat16)
    return (layer_out, new_state)
```

```python
import math

import jax
import jax.numpy as jnp
from jax import lax
from jax.sharding import PartitionSpec as P

EPS = 1e-05


def from_everyone(x, axis):
    copies = jnp.broadcast_to(x, (lax.axis_size(axis), *x.shape))
    return lax.all_to_all(copies, axis, split_axis=0, concat_axis=0, tiled=True)


def in_order(pieces, dim):
    shape = list(pieces.shape[1:])
    shape[dim] *= pieces.shape[0]
    return jnp.moveaxis(pieces, 0, dim).reshape(shape)


def gathered_copies(x, axis, dim):
    pieces = from_everyone(x, axis)
    return in_order(pieces, dim)


def cut_along(x, dim, size):
    shape = x.shape
    pieces = x.reshape(*shape[:dim], size, shape[dim] // size, *shape[dim + 1 :])
    return jnp.moveaxis(pieces, dim, 0)


def sent_and_summed(x, axis, dim):
    size = lax.axis_size(axis)
    pieces = lax.all_to_all(cut_along(x.astype(jnp.bfloat16), dim, size), axis, 0, 0, tiled=True)
    return jnp.sum(pieces.astype(jnp.float32), axis=0)


def in_one_piece(arrays, axis, dim, along):
    widths = [math.prod(a.shape[along:]) for a in arrays]
    both = jnp.concatenate(
        [a.reshape(*a.shape[:along], w) for a, w in zip(arrays, widths)], axis=along
    )
    out = sent_and_summed(both, axis, dim)
    pieces = jnp.split(out, [sum(widths[:k]) for k in range(1, len(widths))], axis=along)
    return tuple((b.reshape(*out.shape[:along], *a.shape[along:]) for a, b in zip(arrays, pieces)))


def project_in(shard_rows, norm_gain, weight_joined, width):
    rows_all = gathered_copies(shard_rows, "tp", 0)
    values = rows_all.astype(jnp.float32)
    squares = jnp.sum(values * values, axis=1)
    normed = (values * norm_gain).astype(jnp.bfloat16)
    product = jnp.dot(normed, weight_joined, preferred_element_type=jnp.float32)
    sums, totals = in_one_piece((product, squares), "kv", 0, 1)
    sums = sums * lax.rsqrt(totals / width + EPS)[:, None]
    return (rows_all, sums)


def project_back(shard_rows, weight):
    return jnp.dot(gathered_copies(shard_rows, "kv", 0), weight, preferred_element_type=jnp.float32)


def sum_widths(terms):
    return sent_and_summed(terms, "tp", 0)


def body(
    tokens,
    state,
    mix_gain,
    q_weight,
    forget_weight,
    input_weight,
    gate_weight,
    lower_bound,
    head_gain,
    out_weight,
    ffn_gain,
    ffn_gate,
    ffn_up,
    ffn_down,
):
    width = tokens.shape[1] * lax.axis_size("kv")
    mixer_joined = jnp.concatenate((q_weight, forget_weight, input_weight, gate_weight), axis=1)
    ffn_joined = jnp.concatenate((ffn_gate, ffn_up), axis=1)
    whole_tokens, mixer_sums = project_in(tokens, mix_gain, mixer_joined, width)
    head_cols = q_weight.shape[1]
    seq_rows = mixer_sums.shape[0]
    heads_here = state.shape[1]
    head_size = state.shape[2]
    split_shape = (seq_rows, heads_here, head_size)
    query = (jax.nn.silu(mixer_sums[:, :head_cols]) * head_size ** (-0.5)).reshape(split_shape)
    forget = lower_bound + (1.0 - lower_bound) * jax.nn.sigmoid(
        mixer_sums[:, head_cols : 2 * head_cols]
    )
    forget = forget.reshape(split_shape)
    value = mixer_sums[:, 2 * head_cols : 3 * head_cols].reshape(split_shape)
    gate_pre = mixer_sums[:, 3 * head_cols :]
    new_state = forget[..., None] * state + (1.0 - forget)[..., None] * value[:, :, None, :]
    read = jnp.einsum("bhk,bhkv->bhv", query, new_state)
    read = read * lax.rsqrt(jnp.mean(read * read, axis=-1, keepdims=True) + EPS) * head_gain
    gated = (read.reshape(seq_rows, head_cols) * jax.nn.silu(gate_pre)).astype(jnp.bfloat16)
    attended_terms = project_back(gated, out_weight)
    attended = sum_widths(attended_terms)
    own_rows = (tokens.astype(jnp.float32) + attended).astype(jnp.bfloat16)
    unused_rows, ffn_sums = project_in(own_rows, ffn_gain, ffn_joined, width)
    ffn_cols = ffn_gate.shape[1]
    hidden = (jax.nn.silu(ffn_sums[:, :ffn_cols]) * ffn_sums[:, ffn_cols:]).astype(jnp.bfloat16)
    layer_out = (own_rows.astype(jnp.float32) + sum_widths(project_back(hidden, ffn_down))).astype(
        jnp.bfloat16
    )
    return (layer_out, new_state)


def solution(mesh):
    in_specs = (
        P("tp", "kv"),
        P("kv", "tp", None, None),
        P("kv"),
        P("kv", "tp"),
        P("kv", "tp"),
        P("kv", "tp"),
        P("kv", "tp"),
        P("tp"),
        P(),
        P("tp", "kv"),
        P("kv"),
        P("kv", "tp"),
        P("kv", "tp"),
        P("tp", "kv"),
    )
    out_specs = (P("tp", "kv"), P("kv", "tp", None, None))
    return jax.shard_map(body, mesh=mesh, in_specs=in_specs, out_specs=out_specs, check_vma=False)
```

```python
import functools

import jax
import jax.numpy as jnp
from jax import lax
from jax.experimental import pallas as pl
from jax.experimental.pallas import tpu as pltpu
from jax.sharding import PartitionSpec as P

EPS = 1e-05
MESH = pl.DeviceIdType.MESH
F32 = jnp.float32
BF16 = jnp.bfloat16


def layer(
    n,
    nx,
    nz,
    width,
    tokens,
    state_in,
    mix_gain,
    lower_bound,
    head_gain,
    ffn_gain,
    wq_in,
    wf_in,
    wi_in,
    wg_in,
    wo_in,
    wfg_in,
    wfu_in,
    wfd_in,
    out,
    state_out,
    w_mix,
    w_out,
    w_ffn,
    w_down,
    state,
    x1,
    s2,
    r2,
    sq_s2,
    sq_r2,
    acc2,
    read_rows,
    gated,
    g3,
    s4,
    r4,
    own,
    x5,
    s6,
    r6,
    sq_s6,
    sq_r6,
    acc6,
    hidden,
    h7,
    s8,
    r8,
    w_sem,
    st_sem,
    so_sem,
    send_sem,
    sq_send_sem,
    x1_sem,
    r2_sem,
    q2_sem,
    g3_sem,
    r4_sem,
    x5_sem,
    r6_sem,
    q6_sem,
    h7_sem,
    r8_sem,
):
    kv = lax.axis_index("kv")
    tp = lax.axis_index("tp")
    ny = n // nx
    rows, cols = tokens.shape
    heads, head = state.shape[1], state.shape[2]

    def kv_peer(j):
        x = (kv % nx + nx // 2 + nx - j % nx) % nx
        y = (kv // nx + ny // 2 + ny - j // nx) % ny
        return y * nx + x

    def tp_peer(j):
        z = (tp // 2 + nz // 2 + nz - j // 2) % nz
        core = (tp % 2 + 1 + j) % 2
        return z * 2 + core

    def kv_source(j):
        x = (kv % nx + nx // 2 + j % nx) % nx
        y = (kv // nx + ny // 2 + j // nx) % ny
        return y * nx + x

    def tp_source(j):
        z = (tp // 2 + nz // 2 + j // 2) % nz
        core = (tp % 2 + 1 + j) % 2
        return z * 2 + core

    axes = {
        "kv": (kv, kv_peer, kv_source, lambda p: (p, tp)),
        "tp": (tp, tp_peer, tp_source, lambda p: (kv, p)),
    }

    def loop(body):
        lax.fori_loop(0, n, lambda j, c: (body(j), c)[1], 0)

    barrier = pltpu.get_barrier_semaphore()

    def greet(j):
        for me, peer_of, _, place in axes.values():
            peer = peer_of(j)

            @pl.when(peer != me)
            def _():
                pl.semaphore_signal(
                    barrier, inc=1, device_id=place(peer), device_id_type=MESH
                )

    loop(greet)

    side = wq_in.shape[1]
    up = wfg_in.shape[1]
    loads = [
        (wq_in, w_mix.at[:, pl.ds(0, side)]),
        (wf_in, w_mix.at[:, pl.ds(side, side)]),
        (wi_in, w_mix.at[:, pl.ds(2 * side, side)]),
        (wg_in, w_mix.at[:, pl.ds(3 * side, side)]),
        (wo_in, w_out),
        (wfg_in, w_ffn.at[:, pl.ds(0, up)]),
        (wfu_in, w_ffn.at[:, pl.ds(up, up)]),
        (wfd_in, w_down),
    ]
    loads = [pltpu.make_async_copy(a, b, w_sem.at[i]) for i, (a, b) in enumerate(loads)]
    for copy in loads:
        copy.start()
    state_load = pltpu.make_async_copy(state_in, state, st_sem)
    state_load.start()

    pl.semaphore_wait(barrier, 2 * (n - 1))

    def send(axis, source, target, phase_sem, recv_sem, peer):
        me, _, _, place = axes[axis]

        @pl.when(peer != me)
        def _():
            pltpu.make_async_remote_copy(
                src_ref=source,
                dst_ref=target.at[me],
                send_sem=phase_sem,
                recv_sem=recv_sem.at[me],
                device_id=place(peer),
                device_id_type=MESH,
            ).start()

        @pl.when(peer == me)
        def _():
            pltpu.make_async_copy(source, target.at[me], recv_sem.at[me]).start()

    def arrived(target, recv_sem, who):
        pltpu.make_async_copy(target.at[who], target.at[who], recv_sem.at[who]).wait()

    def gather(axis, source, target, phase, recv_sem):
        peer_of = axes[axis][1]
        loop(lambda j: send(axis, source, target, send_sem.at[phase], recv_sem, peer_of(j)))

    def add_up(axis, target, recv_sem, total):
        source_of = axes[axis][2]
        total[...] = jnp.zeros_like(total)

        def step(j):
            who = source_of(j)
            arrived(target, recv_sem, who)
            total[...] += target[who].astype(F32)

        loop(step)

    def projected(x, x_sem, gain, weight, s, r, r_sem, sq_s, sq_r, q_sem, phase):
        ones = jnp.ones((8, cols), F32)

        def step(j):
            who = kv_peer(j)
            arrived(x, x_sem, who)
            values = x[who].astype(F32)
            normed = (values * gain[...]).astype(BF16)
            s[who] = jnp.dot(normed, weight[...], preferred_element_type=F32).astype(BF16)
            send("kv", s.at[who], r, send_sem.at[phase], r_sem, who)
            squares = lax.dot_general(
                ones,
                values * values,
                (((1,), (1,)), ((), ())),
                precision=lax.Precision.HIGHEST,
                preferred_element_type=F32,
            )
            sq_s[who, :, pl.ds(0, rows)] = squares[0:1]
            send("kv", sq_s.at[who], sq_r, sq_send_sem.at[phase], q_sem, who)

        sq_s[...] = jnp.zeros_like(sq_s)
        loop(step)

    def factor(sq_r, q_sem):
        def step(j, total):
            who = kv_source(j)
            arrived(sq_r, q_sem, who)
            return total + sq_r[who]

        total = lax.fori_loop(0, n, step, jnp.zeros((1, 128), F32))
        row = lax.rsqrt(total * (1.0 / width) + EPS)
        return jnp.transpose(jnp.broadcast_to(row, (128, 128)))[0:rows]

    def back(g, g_sem, weight, s, r, r_sem, phase):
        def step(j):
            who = tp_peer(j)
            arrived(g, g_sem, who)
            s[who] = jnp.dot(g[who], weight[...], preferred_element_type=F32).astype(BF16)
            send("tp", s.at[who], r, send_sem.at[phase], r_sem, who)

        loop(step)

    gather("tp", tokens, x1, 0, x1_sem)
    for copy in loads[0:4]:
        copy.wait()
    projected(x1, x1_sem, mix_gain, w_mix, s2, r2, r2_sem, sq_s2, sq_r2, q2_sem, 1)
    add_up("kv", r2, r2_sem, acc2)
    scale = factor(sq_r2, q2_sem)

    state_load.wait()
    for h in range(heads):
        q_at = pl.ds(h * head, head)
        f_at = pl.ds(side + h * head, head)
        v_at = pl.ds(2 * side + h * head, head)
        query_pre = acc2[:, q_at] * scale
        acc2[:, q_at] = query_pre * jax.nn.sigmoid(query_pre) * (head ** (-0.5))
        low = lower_bound[:, q_at]
        acc2[:, f_at] = low + (1.0 - low) * jax.nn.sigmoid(acc2[:, f_at] * scale)
        acc2[:, v_at] = acc2[:, v_at] * scale

    def state_out_copy(group):
        at = pl.ds(group * 8, 8)
        return pltpu.make_async_copy(state.at[at], state_out.at[at], so_sem)

    def eight(group, carry):
        first = pl.multiple_of(group * 8, 8)
        for h in range(heads):
            eight_rows = pl.ds(first, 8)
            query = jnp.transpose(acc2[eight_rows, pl.ds(h * head, head)])
            forget = jnp.transpose(acc2[eight_rows, pl.ds(side + h * head, head)])
            value = acc2[eight_rows, pl.ds(2 * side + h * head, head)]
            reads = []
            for b in range(8):
                v = value[b : b + 1]
                new = v + forget[:, b : b + 1] * (state[first + b, h] - v)
                state[first + b, h] = new
                reads.append(jnp.sum(query[:, b : b + 1] * new, axis=0, keepdims=True))
            read_rows[eight_rows, pl.ds(h * head, head)] = jnp.concatenate(reads, axis=0)
        state_out_copy(group).start()
        return carry

    lax.fori_loop(0, rows // 8, eight, 0)

    for h in range(heads):
        at = pl.ds(h * head, head)
        read = read_rows[:, at]
        mean = jnp.mean(read * read, axis=-1, keepdims=True)
        read = read * lax.rsqrt(mean + EPS) * head_gain[...]
        gate = acc2[:, pl.ds(3 * side + h * head, head)] * scale
        gated[:, at] = (read * (gate * jax.nn.sigmoid(gate))).astype(BF16)

    gather("kv", gated, g3, 2, g3_sem)
    loads[4].wait()
    back(g3, g3_sem, w_out, s4, r4, r4_sem, 3)
    add_up("tp", r4, r4_sem, read_rows)
    own[...] = (tokens[...].astype(F32) + read_rows[...]).astype(BF16)

    gather("tp", own, x5, 4, x5_sem)
    loads[5].wait()
    loads[6].wait()
    projected(x5, x5_sem, ffn_gain, w_ffn, s6, r6, r6_sem, sq_s6, sq_r6, q6_sem, 5)
    add_up("kv", r6, r6_sem, acc6)
    scale = factor(sq_r6, q6_sem)
    for c in range(up // 128):
        at = pl.ds(c * 128, 128)
        gate = acc6[:, at] * scale
        hidden[:, at] = (
            gate * jax.nn.sigmoid(gate) * (acc6[:, pl.ds(up + c * 128, 128)] * scale)
        ).astype(BF16)
    gather("kv", hidden, h7, 6, h7_sem)
    loads[7].wait()
    back(h7, h7_sem, w_down, s8, r8, r8_sem, 7)
    add_up("tp", r8, r8_sem, read_rows)
    out[...] = (own[...].astype(F32) + read_rows[...]).astype(BF16)

    for phase, buffer in enumerate((x1, r2, g3, r4, x5, r6, h7, r8)):
        sent = buffer.at[pl.ds(0, n - 1)]
        pltpu.make_async_copy(sent, sent, send_sem.at[phase]).wait()
    for phase, buffer in ((1, sq_r2), (5, sq_r6)):
        sent = buffer.at[pl.ds(0, n - 1)]
        pltpu.make_async_copy(sent, sent, sq_send_sem.at[phase]).wait()
    pltpu.make_async_copy(state, state_out, so_sem).wait()


def body(
    tokens,
    state,
    mix_gain,
    q_weight,
    forget_weight,
    input_weight,
    gate_weight,
    lower_bound,
    head_gain,
    out_weight,
    ffn_gain,
    ffn_gate,
    ffn_up,
    ffn_down,
):
    n = lax.axis_size("kv")
    nx, nz = {16: (4, 8), 4: (2, 2)}[n]
    rows, cols = tokens.shape
    side, up = q_weight.shape[1], ffn_gate.shape[1]
    vmem, dma = pltpu.VMEM, pltpu.SemaphoreType.DMA
    in_vmem = pl.BlockSpec(memory_space=pltpu.VMEM)
    in_hbm = pl.BlockSpec(memory_space=pl.ANY)
    narrow = (n, rows, cols)
    return pl.pallas_call(
        functools.partial(layer, n, nx, nz, cols * n),
        out_shape=(
            jax.ShapeDtypeStruct(tokens.shape, BF16),
            jax.ShapeDtypeStruct(state.shape, F32),
        ),
        in_specs=[in_vmem, in_hbm, in_vmem, in_vmem, in_vmem, in_vmem] + [in_hbm] * 8,
        out_specs=(in_vmem, in_hbm),
        scratch_shapes=[
            vmem((cols, 4 * side), BF16),
            vmem(out_weight.shape, BF16),
            vmem((cols, 2 * up), BF16),
            vmem(ffn_down.shape, BF16),
            vmem(state.shape, F32),
            vmem(narrow, BF16),
            vmem((n, rows, 4 * side), BF16),
            vmem((n, rows, 4 * side), BF16),
            vmem((n, 1, 128), F32),
            vmem((n, 1, 128), F32),
            vmem((rows, 4 * side), F32),
            vmem((rows, side), F32),
            vmem((rows, side), BF16),
            vmem((n, rows, side), BF16),
            vmem(narrow, BF16),
            vmem(narrow, BF16),
            vmem((rows, cols), BF16),
            vmem(narrow, BF16),
            vmem((n, rows, 2 * up), BF16),
            vmem((n, rows, 2 * up), BF16),
            vmem((n, 1, 128), F32),
            vmem((n, 1, 128), F32),
            vmem((rows, 2 * up), F32),
            vmem((rows, up), BF16),
            vmem((n, rows, up), BF16),
            vmem(narrow, BF16),
            vmem(narrow, BF16),
            dma((8,)),
            dma,
            dma,
            dma((8,)),
            dma((8,)),
        ]
        + [dma((n,))] * 10,
        compiler_params=pltpu.CompilerParams(collective_id=0, has_side_effects=True),
        name="layer",
    )(
        tokens,
        state,
        mix_gain.reshape(1, -1),
        lower_bound.reshape(1, -1),
        head_gain.reshape(1, -1),
        ffn_gain.reshape(1, -1),
        q_weight,
        forget_weight,
        input_weight,
        gate_weight,
        out_weight,
        ffn_gate,
        ffn_up,
        ffn_down,
    )


def solution(mesh):
    in_specs = (
        P("tp", "kv"),
        P("kv", "tp", None, None),
        P("kv"),
        P("kv", "tp"),
        P("kv", "tp"),
        P("kv", "tp"),
        P("kv", "tp"),
        P("tp"),
        P(),
        P("tp", "kv"),
        P("kv"),
        P("kv", "tp"),
        P("kv", "tp"),
        P("tp", "kv"),
    )
    out_specs = (P("tp", "kv"), P("kv", "tp", None, None))
    return jax.shard_map(body, mesh=mesh, in_specs=in_specs, out_specs=out_specs, check_vma=False)
```

```python
import functools

import jax
import jax.numpy as jnp
from jax import lax
from jax.experimental import pallas as pl
from jax.experimental.pallas import tpu as pltpu
from jax.sharding import PartitionSpec as P

EPS = 1e-05
MESH = pl.DeviceIdType.MESH
F32 = jnp.float32
BF16 = jnp.bfloat16
HEAD = 128
EARLY = False


def ffn_chunks(up):
    first = (up // 256 + 1) * 128
    return ((0, first), (first, up - first))


def layer(n, nx, nz, width, *refs):
    (
        tokens,
        state_in,
        mix_gain,
        lower_bound,
        head_gain,
        ffn_gain,
        wq_in,
        wf_in,
        wi_in,
        wg_in,
        wo_in,
        wfg_in,
        wfu_in,
        wfd_in,
        out,
        forget_out,
        value_out,
        w_mix,
        w_out,
        w_ffn,
        w_down,
        state,
        x1,
        s2a,
        s2b,
        r2a,
        r2b,
        sq_s2,
        sq_r2,
        acc2,
        total,
        gated,
        g3,
        o4,
        p4,
        m4,
        s4,
        r4,
        own,
        x5,
        s6a,
        s6b,
        r6a,
        r6b,
        sq_s6,
        sq_r6,
        acc6a,
        acc6b,
        hida,
        hidb,
        h7a,
        h7b,
        o8,
        p8,
        m8,
        s8,
        r8,
        w_sem,
        st_sem,
        send_sem,
        x1_sem,
        r2a_sem,
        r2b_sem,
        q2_sem,
        g3_sem,
        p4_sem,
        r4_sem,
        x5_sem,
        r6a_sem,
        r6b_sem,
        q6_sem,
        h7a_sem,
        h7b_sem,
        p8_sem,
        r8_sem,
    ) = refs
    kv = lax.axis_index("kv")
    tp = lax.axis_index("tp")
    z, core = tp // 2, tp % 2
    mate = z * 2 + 1 - core
    ny = n // nx
    rows, cols = tokens.shape
    side = wq_in.shape[1]
    up = wfg_in.shape[1]
    heads = side // HEAD
    drains = []

    def kv_peer(j):
        x = (kv % nx + nx // 2 + nx - j % nx) % nx
        y = (kv // nx + ny // 2 + ny - j // nx) % ny
        return y * nx + x

    def kv_source(j):
        x = (kv % nx + nx // 2 + j % nx) % nx
        y = (kv // nx + ny // 2 + j // nx) % ny
        return y * nx + x

    def z_near(i):
        return (z + nz + jnp.where(i % 2 == 1, (i + 1) // 2, -(i // 2))) % nz

    def z_far(i):
        return z_near(nz - 1 - i)

    def loop(count, body):
        lax.fori_loop(0, count, lambda j, c: (body(j), c)[1], 0)

    barrier = pltpu.get_barrier_semaphore()

    def greet(who):
        pl.semaphore_signal(barrier, inc=1, device_id=who, device_id_type=MESH)

    @functools.partial(loop, n)
    def _(j):
        peer = kv_peer(j)

        @pl.when(peer != kv)
        def _():
            greet((peer, tp))

    @functools.partial(loop, nz - 1)
    def _(i):
        greet((kv, z_far(i) * 2 + core))

    greet((kv, mate))

    loads = []
    for h in range(heads):
        for k, w in enumerate((wq_in, wf_in, wi_in, wg_in)):
            loads.append(
                (w.at[:, pl.ds(h * HEAD, HEAD)], w_mix.at[:, pl.ds((4 * h + k) * HEAD, HEAD)])
            )
    n_mix = len(loads)
    loads.append((wo_in, w_out))
    for first, size in ffn_chunks(up):
        loads.append((wfg_in.at[:, pl.ds(first, size)], w_ffn.at[:, pl.ds(2 * first, size)]))
        loads.append((wfu_in.at[:, pl.ds(first, size)], w_ffn.at[:, pl.ds(2 * first + size, size)]))
    loads.append((wfd_in, w_down))
    loads = [pltpu.make_async_copy(a, b, w_sem.at[i]) for i, (a, b) in enumerate(loads)]
    for copy in loads:
        copy.start()
    state_load = pltpu.make_async_copy(state_in, state, st_sem)
    state_load.start()

    pl.semaphore_wait(barrier, (n - 1) + (nz - 1) + 1)

    def push(source, target, where, sent, landed, device):
        pltpu.make_async_remote_copy(
            src_ref=source,
            dst_ref=target.at[where],
            send_sem=sent,
            recv_sem=landed.at[where],
            device_id=device,
            device_id_type=MESH,
        ).start()

    def arrived(target, landed, who):
        pltpu.make_async_copy(target.at[who], target.at[who], landed.at[who]).wait()

    def to_kv(source, target, sent, landed, peer):
        @pl.when(peer != kv)
        def _():
            push(source, target, kv, sent, landed, (peer, tp))

        @pl.when(peer == kv)
        def _():
            pltpu.make_async_copy(source, target.at[kv], landed.at[kv]).start()

    def gather_kv(source, target, slot, landed):
        loop(n, lambda j: to_kv(source, target, send_sem.at[slot], landed, kv_peer(j)))
        drains.append((target, n - 1, slot))

    def gather_tp(source, target, slot, landed):
        target[tp] = source[...]
        sent = send_sem.at[slot]
        loop(
            nz - 1, lambda i: push(source, target, tp, sent, landed, (kv, z_far(i) * 2 + core))
        )
        push(source, target, tp, sent, landed, (kv, mate))
        drains.append((target, n - 1, slot))

    def projected(x, x_sem, x_slot, gain, weight, parts, sq_s, sq_r, q_sem, q_slot):
        ones = jnp.ones((8, cols), F32)
        sq_s[...] = jnp.zeros_like(sq_s)

        def step(i):
            @pl.when(i < nz)
            def _():
                here = z_near(i) * 2 + core

                @pl.when(i > 0)
                def _():
                    arrived(x, x_sem, here)
                    push(x.at[here], x, here, send_sem.at[x_slot], x_sem, (kv, mate))

            @pl.when(i > 0)
            def _():
                chip = z_near(i - 1)
                arrived(x, x_sem, chip * 2 + 1 - core)
                pair = pl.ds(chip * 2, 2)
                values = x[pair].reshape(2 * rows, cols).astype(F32)
                normed = (values * gain[...]).astype(BF16)
                for s, _, _, _, first, size in parts:
                    product = jnp.dot(
                        normed, weight[:, pl.ds(first, size)], preferred_element_type=F32
                    )
                    s[pair] = product.astype(BF16).reshape(2, rows, size)
                squares = lax.dot_general(
                    ones,
                    values * values,
                    (((1,), (1,)), ((), ())),
                    precision=lax.Precision.HIGHEST,
                    preferred_element_type=F32,
                )
                for k in range(2):
                    sq_s[chip * 2 + k, :, pl.ds(0, rows)] = squares[0:1, k * rows : (k + 1) * rows]
                if EARLY:
                    s, r, landed, slot, _, _ = parts[0]
                    for k in range(2):
                        peer = chip * 2 + (kv + k) % 2
                        to_kv(s.at[peer], r, send_sem.at[slot], landed, peer)

        loop(nz + 1, step)
        for p, (s, r, landed, slot, _, _) in enumerate(parts):

            def send(j):
                peer = kv_peer(j)
                if p > 0 or not EARLY:
                    to_kv(s.at[peer], r, send_sem.at[slot], landed, peer)
                if p == 0:
                    to_kv(sq_s.at[peer], sq_r, send_sem.at[q_slot], q_sem, peer)

            loop(n, send)
            drains.append((r, n - 1, slot))
        drains.append((sq_r, n - 1, q_slot))

    def add_up(count, source_of, target, landed, into):
        into[...] = jnp.zeros_like(into)

        def step(j):
            who = source_of(j)
            arrived(target, landed, who)
            into[...] += target[who].astype(F32)

        loop(count, step)

    def factor(sq_r, q_sem):
        def step(j, sums):
            who = kv_source(j)
            arrived(sq_r, q_sem, who)
            return sums + sq_r[who]

        sums = lax.fori_loop(0, n, step, jnp.zeros((1, 128), F32))
        row = lax.rsqrt(sums * (1.0 / width) + EPS)
        return jnp.transpose(jnp.broadcast_to(row, (128, 128)))[0:rows]

    def back(gs, weight, o, p, p_sem, p_slot, m, s, r, r_sem, r_slot):
        def step(i):
            @pl.when(i < nz)
            def _():
                chip = z_far(i)
                pair = pl.ds(chip * 2, 2)
                product = None
                for g, landed, first in gs:
                    arrived(g, landed, chip * 2)
                    arrived(g, landed, chip * 2 + 1)
                    size = g.shape[2]
                    term = jnp.dot(
                        g[pair].reshape(2 * rows, size),
                        weight[pl.ds(first, size), :],
                        preferred_element_type=F32,
                    )
                    product = term if product is None else product + term
                low, high = product[0:rows], product[rows : 2 * rows]
                o[chip] = jnp.where(core == 0, high, low).astype(BF16)
                push(o.at[chip], p, chip, send_sem.at[p_slot], p_sem, (kv, mate))
                m[chip] = jnp.where(core == 0, low, high)

            @pl.when(i > 0)
            def _():
                chip = z_far(i - 1)
                arrived(p, p_sem, chip)
                s[chip] = (m[chip] + p[chip].astype(F32)).astype(BF16)

                @pl.when(chip != z)
                def _():
                    push(s.at[chip], r, z, send_sem.at[r_slot], r_sem, (kv, chip * 2 + core))

                @pl.when(chip == z)
                def _():
                    pltpu.make_async_copy(s.at[chip], r.at[z], r_sem.at[z]).start()

        loop(nz + 1, step)
        drains.append((p, nz, p_slot))
        drains.append((r, nz - 1, r_slot))

    gather_tp(tokens, x1, 0, x1_sem)
    for copy in loads[0:n_mix]:
        copy.wait()
    parts = [
        (s2a, r2a, r2a_sem, 1, 0, 4 * HEAD),
        (s2b, r2b, r2b_sem, 2, 4 * HEAD, 4 * HEAD),
    ]
    projected(x1, x1_sem, 0, mix_gain, w_mix, parts, sq_s2, sq_r2, q2_sem, 3)

    scale = factor(sq_r2, q2_sem)
    state_load.wait()
    for h in range(heads):
        at = pl.ds(h * HEAD, HEAD)
        add_up(n, kv_source, (r2a, r2b)[h], (r2a_sem, r2b_sem)[h], acc2)
        query = acc2[:, 0:HEAD] * scale
        query = query * jax.nn.sigmoid(query) * (HEAD ** (-0.5))
        low = lower_bound[:, at]
        forget = low + (1.0 - low) * jax.nn.sigmoid(acc2[:, HEAD : 2 * HEAD] * scale)
        value = acc2[:, 2 * HEAD : 3 * HEAD] * scale
        gate = acc2[:, 3 * HEAD : 4 * HEAD] * scale
        forget_out[:, at] = forget
        value_out[:, at] = value
        kept = query * forget
        added = jnp.sum(query - kept, axis=-1, keepdims=True) * value
        acc2[:, 0:HEAD] = kept

        def eight(group, carry):
            eight_rows = pl.ds(pl.multiple_of(group * 8, 8), 8)
            columns = jnp.transpose(acc2[eight_rows, 0:HEAD])
            reads = []
            for b in range(8):
                reads.append(
                    jnp.sum(
                        columns[:, b : b + 1] * state[group * 8 + b, h], axis=0, keepdims=True
                    )
                )
            total[eight_rows, 0:HEAD] = jnp.concatenate(reads, axis=0)
            return carry

        lax.fori_loop(0, rows // 8, eight, 0)
        read = total[:, 0:HEAD] + added
        mean = jnp.mean(read * read, axis=-1, keepdims=True)
        read = read * lax.rsqrt(mean + EPS) * head_gain[...]
        gated[:, at] = (read * (gate * jax.nn.sigmoid(gate))).astype(BF16)

    gather_kv(gated, g3, 4, g3_sem)
    loads[n_mix].wait()
    back([(g3, g3_sem, 0)], w_out, o4, p4, p4_sem, 5, m4, s4, r4, r4_sem, 6)
    add_up(nz, z_near, r4, r4_sem, total)
    own[...] = (tokens[...].astype(F32) + total[...]).astype(BF16)

    gather_tp(own, x5, 7, x5_sem)
    for copy in loads[n_mix + 1 : -1]:
        copy.wait()
    (a_at, a_size), (b_at, b_size) = ffn_chunks(up)
    parts = [
        (s6a, r6a, r6a_sem, 8, 2 * a_at, 2 * a_size),
        (s6b, r6b, r6b_sem, 9, 2 * b_at, 2 * b_size),
    ]
    projected(x5, x5_sem, 7, ffn_gain, w_ffn, parts, sq_s6, sq_r6, q6_sem, 10)
    scale = factor(sq_r6, q6_sem)
    for r, landed, acc, hid, h7, h7_sem, slot in (
        (r6a, r6a_sem, acc6a, hida, h7a, h7a_sem, 11),
        (r6b, r6b_sem, acc6b, hidb, h7b, h7b_sem, 12),
    ):
        add_up(n, kv_source, r, landed, acc)
        size = hid.shape[1]
        for c in range(size // 128):
            gate = acc[:, c * 128 : (c + 1) * 128] * scale
            upper = acc[:, size + c * 128 : size + (c + 1) * 128] * scale
            hid[:, c * 128 : (c + 1) * 128] = (gate * jax.nn.sigmoid(gate) * upper).astype(BF16)
        gather_kv(hid, h7, slot, h7_sem)
    loads[-1].wait()
    gs = [(h7a, h7a_sem, a_at), (h7b, h7b_sem, b_at)]
    back(gs, w_down, o8, p8, p8_sem, 13, m8, s8, r8, r8_sem, 14)
    add_up(nz, z_near, r8, r8_sem, total)
    out[...] = (own[...].astype(F32) + total[...]).astype(BF16)

    for target, count, slot in drains:
        sent = target.at[pl.ds(0, count)]
        pltpu.make_async_copy(sent, sent, send_sem.at[slot]).wait()


def update(rows_in, forget, value, state, rows_out, state_out):
    rows_out[...] = rows_in[...]
    for h in range(state.shape[1]):
        columns = jnp.transpose(forget[:, h * HEAD : (h + 1) * HEAD])
        for b in range(8):
            v = value[b : b + 1, h * HEAD : (h + 1) * HEAD]
            state_out[b, h] = v + columns[:, b : b + 1] * (state[b, h] - v)


def body(
    tokens,
    state,
    mix_gain,
    q_weight,
    forget_weight,
    input_weight,
    gate_weight,
    lower_bound,
    head_gain,
    out_weight,
    ffn_gain,
    ffn_gate,
    ffn_up,
    ffn_down,
):
    n = lax.axis_size("kv")
    nx, nz = {16: (4, 8), 4: (2, 2)}[n]
    rows, cols = tokens.shape
    side, up = q_weight.shape[1], ffn_gate.shape[1]
    vmem, dma = pltpu.VMEM, pltpu.SemaphoreType.DMA
    in_vmem = pl.BlockSpec(memory_space=pltpu.VMEM)
    in_hbm = pl.BlockSpec(memory_space=pl.ANY)
    block = (rows, cols)
    all_blocks = vmem((n, *block), BF16)
    all_heads = vmem((n, rows, 4 * HEAD), BF16)
    chip_blocks = vmem((nz, *block), BF16)
    chip_sums = vmem((nz, *block), F32)
    squares = vmem((n, 1, 128), F32)
    (_, a_size), (_, b_size) = ffn_chunks(up)
    backward = [chip_blocks, chip_blocks, chip_sums, chip_blocks, chip_blocks]
    layer_out, forget, value = pl.pallas_call(
        functools.partial(layer, n, nx, nz, cols * n),
        out_shape=(
            jax.ShapeDtypeStruct(block, BF16),
            jax.ShapeDtypeStruct(block, F32),
            jax.ShapeDtypeStruct(block, F32),
        ),
        in_specs=[in_vmem, in_hbm, in_vmem, in_vmem, in_vmem, in_vmem] + [in_hbm] * 8,
        out_specs=(in_vmem, in_vmem, in_vmem),
        scratch_shapes=[
            vmem((cols, 4 * side), BF16),
            vmem(out_weight.shape, BF16),
            vmem((cols, 2 * up), BF16),
            vmem(ffn_down.shape, BF16),
            vmem(state.shape, F32),
            all_blocks,
            all_heads,
            all_heads,
            all_heads,
            all_heads,
            squares,
            squares,
            vmem((rows, 4 * HEAD), F32),
            vmem(block, F32),
            vmem(block, BF16),
            all_blocks,
            *backward,
            vmem(block, BF16),
            all_blocks,
            vmem((n, rows, 2 * a_size), BF16),
            vmem((n, rows, 2 * b_size), BF16),
            vmem((n, rows, 2 * a_size), BF16),
            vmem((n, rows, 2 * b_size), BF16),
            squares,
            squares,
            vmem((rows, 2 * a_size), F32),
            vmem((rows, 2 * b_size), F32),
            vmem((rows, a_size), BF16),
            vmem((rows, b_size), BF16),
            vmem((n, rows, a_size), BF16),
            vmem((n, rows, b_size), BF16),
            *backward,
            dma((4 * (side // HEAD) + 6,)),
            dma,
            dma((15,)),
            dma((n,)),
            dma((n,)),
            dma((n,)),
            dma((n,)),
            dma((n,)),
            dma((nz,)),
            dma((nz,)),
            dma((n,)),
            dma((n,)),
            dma((n,)),
            dma((n,)),
            dma((n,)),
            dma((n,)),
            dma((nz,)),
            dma((nz,)),
        ],
        compiler_params=pltpu.CompilerParams(collective_id=0, has_side_effects=True),
        name="layer",
    )(
        tokens,
        state,
        mix_gain.reshape(1, -1),
        lower_bound.reshape(1, -1),
        head_gain.reshape(1, -1),
        ffn_gain.reshape(1, -1),
        q_weight,
        forget_weight,
        input_weight,
        gate_weight,
        out_weight,
        ffn_gate,
        ffn_up,
        ffn_down,
    )
    eight = pl.BlockSpec((8, side), lambda i: (i, 0))
    states = pl.BlockSpec((8, *state.shape[1:]), lambda i: (i, 0, 0, 0))
    return pl.pallas_call(
        update,
        grid=(rows // 8,),
        out_shape=(
            jax.ShapeDtypeStruct(block, BF16),
            jax.ShapeDtypeStruct(state.shape, F32),
        ),
        in_specs=[pl.BlockSpec((8, cols), lambda i: (i, 0)), eight, eight, states],
        out_specs=(pl.BlockSpec((8, cols), lambda i: (i, 0)), states),
        name="update",
    )(layer_out, forget, value, state)


def solution(mesh):
    in_specs = (
        P("tp", "kv"),
        P("kv", "tp", None, None),
        P("kv"),
        P("kv", "tp"),
        P("kv", "tp"),
        P("kv", "tp"),
        P("kv", "tp"),
        P("tp"),
        P(),
        P("tp", "kv"),
        P("kv"),
        P("kv", "tp"),
        P("kv", "tp"),
        P("tp", "kv"),
    )
    out_specs = (P("tp", "kv"), P("kv", "tp", None, None))
    return jax.shard_map(body, mesh=mesh, in_specs=in_specs, out_specs=out_specs, check_vma=False)
```

```python
import functools

import jax
import jax.numpy as jnp
from jax import lax
from jax.experimental import pallas as pl
from jax.experimental.pallas import tpu as pltpu
from jax.sharding import PartitionSpec as P

EPS = 1e-05
MESH = pl.DeviceIdType.MESH
F32 = jnp.float32
BF16 = jnp.bfloat16
HEAD = 128


def ffn_chunks(up):
    first = (up // 256 + 1) * 128
    return ((0, first), (first, up - first))


def layer(n, nx, nz, width, *refs):
    (
        tokens,
        state_in,
        mix_gain,
        lower_bound,
        head_gain,
        ffn_gain,
        wq_in,
        wf_in,
        wi_in,
        wg_in,
        wo_in,
        wfg_in,
        wfu_in,
        wfd_in,
        out,
        state,
        w_mix,
        w_out,
        w_ffn,
        w_down,
        forgets,
        values,
        x1,
        s2a,
        s2b,
        r2a,
        r2b,
        sq_s2,
        sq_r2,
        acc2,
        total,
        gated,
        g3a,
        g3b,
        o4,
        p4,
        m4,
        s4,
        r4,
        own,
        x5,
        s6a,
        s6b,
        r6a,
        r6b,
        sq_s6,
        sq_r6,
        acc6a,
        acc6b,
        hida,
        hidb,
        h7a,
        h7b,
        o8,
        p8,
        m8,
        s8,
        r8,
        w_sem,
        st_sem,
        send_sem,
        x1_sem,
        r2a_sem,
        r2b_sem,
        q2_sem,
        g3a_sem,
        g3b_sem,
        p4_sem,
        r4_sem,
        x5_sem,
        r6a_sem,
        r6b_sem,
        q6_sem,
        h7a_sem,
        h7b_sem,
        p8_sem,
        r8_sem,
    ) = refs
    kv = lax.axis_index("kv")
    tp = lax.axis_index("tp")
    z, core = tp // 2, tp % 2
    mate = z * 2 + 1 - core
    ny = n // nx
    rows, cols = tokens.shape
    side = wq_in.shape[1]
    up = wfg_in.shape[1]
    heads = side // HEAD
    drains = []

    def kv_peer(j):
        x = (kv % nx + nx // 2 + nx - j % nx) % nx
        y = (kv // nx + ny // 2 + ny - j // nx) % ny
        return y * nx + x

    def kv_source(j):
        x = (kv % nx + nx // 2 + j % nx) % nx
        y = (kv // nx + ny // 2 + j // nx) % ny
        return y * nx + x

    def z_near(i):
        return (z + nz + jnp.where(i % 2 == 1, (i + 1) // 2, -(i // 2))) % nz

    def z_far(i):
        return z_near(nz - 1 - i)

    def loop(count, body):
        lax.fori_loop(0, count, lambda j, c: (body(j), c)[1], 0)

    barrier = pltpu.get_barrier_semaphore()

    def greet(who):
        pl.semaphore_signal(barrier, inc=1, device_id=who, device_id_type=MESH)

    @functools.partial(loop, n)
    def _(j):
        peer = kv_peer(j)

        @pl.when(peer != kv)
        def _():
            greet((peer, tp))

    @functools.partial(loop, nz - 1)
    def _(i):
        greet((kv, z_far(i) * 2 + core))

    greet((kv, mate))

    loads = []
    for h in range(heads):
        for k, w in enumerate((wq_in, wf_in, wi_in, wg_in)):
            loads.append(
                (w.at[:, pl.ds(h * HEAD, HEAD)], w_mix.at[:, pl.ds((4 * h + k) * HEAD, HEAD)])
            )
    n_mix = len(loads)
    loads.append((wo_in, w_out))
    for first, size in ffn_chunks(up):
        loads.append((wfg_in.at[:, pl.ds(first, size)], w_ffn.at[:, pl.ds(2 * first, size)]))
        loads.append((wfu_in.at[:, pl.ds(first, size)], w_ffn.at[:, pl.ds(2 * first + size, size)]))
    loads.append((wfd_in, w_down))
    loads = [pltpu.make_async_copy(a, b, w_sem.at[i]) for i, (a, b) in enumerate(loads)]
    for copy in loads:
        copy.start()
    state_load = pltpu.make_async_copy(state_in, state, st_sem)
    state_load.start()

    pl.semaphore_wait(barrier, (n - 1) + (nz - 1) + 1)

    def push(source, target, where, sent, landed, device):
        pltpu.make_async_remote_copy(
            src_ref=source,
            dst_ref=target.at[where],
            send_sem=sent,
            recv_sem=landed.at[where],
            device_id=device,
            device_id_type=MESH,
        ).start()

    def arrived(target, landed, who):
        pltpu.make_async_copy(target.at[who], target.at[who], landed.at[who]).wait()

    def to_kv(source, target, sent, landed, peer):
        @pl.when(peer != kv)
        def _():
            push(source, target, kv, sent, landed, (peer, tp))

        @pl.when(peer == kv)
        def _():
            pltpu.make_async_copy(source, target.at[kv], landed.at[kv]).start()

    def gather_kv(source, target, slot, landed):
        loop(n, lambda j: to_kv(source, target, send_sem.at[slot], landed, kv_peer(j)))
        drains.append((target, n - 1, slot))

    def gather_tp(source, target, slot, landed):
        target[tp] = source[...]
        sent = send_sem.at[slot]
        push(source, target, tp, sent, landed, (kv, mate))
        loop(
            nz - 1,
            lambda i: push(source, target, tp, sent, landed, (kv, z_near(i + 1) * 2 + core)),
        )
        drains.append((target, n - 1, slot))

    def projected(x, x_sem, x_slot, gain, weight, parts, sq_s, sq_r, q_sem, q_slot):
        ones = jnp.ones((8, cols), F32)
        lag = min(2, nz)
        sq_s[...] = jnp.zeros_like(sq_s)

        def step(i):
            @pl.when(i < nz)
            def _():
                here = z_near(i) * 2 + core

                @pl.when(i > 0)
                def _():
                    arrived(x, x_sem, here)
                    push(x.at[here], x, here, send_sem.at[x_slot], x_sem, (kv, mate))

            @pl.when(i >= lag)
            def _():
                chip = z_near(i - lag)
                arrived(x, x_sem, chip * 2 + 1 - core)
                pair = pl.ds(chip * 2, 2)
                values = x[pair].reshape(2 * rows, cols).astype(F32)
                normed = (values * gain[...]).astype(BF16)
                for s, _, _, _, first, size in parts:
                    product = jnp.dot(
                        normed, weight[:, pl.ds(first, size)], preferred_element_type=F32
                    )
                    s[pair] = product.astype(BF16).reshape(2, rows, size)
                squares = lax.dot_general(
                    ones,
                    values * values,
                    (((1,), (1,)), ((), ())),
                    precision=lax.Precision.HIGHEST,
                    preferred_element_type=F32,
                )
                for k in range(2):
                    sq_s[chip * 2 + k, :, pl.ds(0, rows)] = squares[0:1, k * rows : (k + 1) * rows]

        loop(nz + lag, step)
        for p, (s, r, landed, slot, _, _) in enumerate(parts):

            def send(j):
                peer = kv_peer(j)
                to_kv(s.at[peer], r, send_sem.at[slot], landed, peer)
                if p == 0:
                    to_kv(sq_s.at[peer], sq_r, send_sem.at[q_slot], q_sem, peer)

            loop(n, send)
            drains.append((r, n - 1, slot))
        drains.append((sq_r, n - 1, q_slot))

    def add_up(count, source_of, target, landed, into):
        into[...] = jnp.zeros_like(into)

        def step(j):
            who = source_of(j)
            arrived(target, landed, who)
            into[...] += target[who].astype(F32)

        loop(count, step)

    def factor(sq_r, q_sem):
        def step(j, sums):
            who = kv_source(j)
            arrived(sq_r, q_sem, who)
            return sums + sq_r[who]

        sums = lax.fori_loop(0, n, step, jnp.zeros((1, 128), F32))
        row = lax.rsqrt(sums * (1.0 / width) + EPS)
        return jnp.transpose(jnp.broadcast_to(row, (128, 128)))[0:rows]

    def back(gs, weight, o, p, p_sem, p_slot, m, s, r, r_sem, r_slot):
        def multiply(i):
            chip = z_far(i)
            pair = pl.ds(chip * 2, 2)
            product = None
            for g, landed, first in gs:
                arrived(g, landed, chip * 2)
                arrived(g, landed, chip * 2 + 1)
                size = g.shape[2]
                term = jnp.dot(
                    g[pair].reshape(2 * rows, size),
                    weight[pl.ds(first, size), :],
                    preferred_element_type=F32,
                )
                product = term if product is None else product + term
            low, high = product[0:rows], product[rows : 2 * rows]
            o[chip] = jnp.where(core == 0, high, low).astype(BF16)
            push(o.at[chip], p, chip, send_sem.at[p_slot], p_sem, (kv, mate))
            m[chip] = jnp.where(core == 0, low, high)

        def pass_on(i):
            chip = z_far(i)
            arrived(p, p_sem, chip)
            s[chip] = (m[chip] + p[chip].astype(F32)).astype(BF16)

            @pl.when(chip != z)
            def _():
                push(s.at[chip], r, z, send_sem.at[r_slot], r_sem, (kv, chip * 2 + core))

            @pl.when(chip == z)
            def _():
                pltpu.make_async_copy(s.at[chip], r.at[z], r_sem.at[z]).start()

        loop(nz, multiply)
        loop(nz, pass_on)
        drains.append((p, nz, p_slot))
        drains.append((r, nz - 1, r_slot))

    gather_tp(tokens, x1, 0, x1_sem)
    for copy in loads[0:n_mix]:
        copy.wait()
    parts = [
        (s2a, r2a, r2a_sem, 1, 0, 4 * HEAD),
        (s2b, r2b, r2b_sem, 2, 4 * HEAD, 4 * HEAD),
    ]
    projected(x1, x1_sem, 0, mix_gain, w_mix, parts, sq_s2, sq_r2, q2_sem, 3)

    scale = factor(sq_r2, q2_sem)
    state_load.wait()
    for h in range(heads):
        at = pl.ds(h * HEAD, HEAD)
        add_up(n, kv_source, (r2a, r2b)[h], (r2a_sem, r2b_sem)[h], acc2)
        query = acc2[:, 0:HEAD] * scale
        query = query * jax.nn.sigmoid(query) * (HEAD ** (-0.5))
        low = lower_bound[:, at]
        forget = low + (1.0 - low) * jax.nn.sigmoid(acc2[:, HEAD : 2 * HEAD] * scale)
        value = acc2[:, 2 * HEAD : 3 * HEAD] * scale
        gate = acc2[:, 3 * HEAD : 4 * HEAD] * scale
        forgets[:, at] = forget
        values[:, at] = value
        kept = query * forget
        added = jnp.sum(query - kept, axis=-1, keepdims=True) * value
        acc2[:, 0:HEAD] = kept

        def eight(group, carry):
            eight_rows = pl.ds(pl.multiple_of(group * 8, 8), 8)
            columns = jnp.transpose(acc2[eight_rows, 0:HEAD])
            reads = []
            for b in range(8):
                reads.append(
                    jnp.sum(
                        columns[:, b : b + 1] * state[group * 8 + b, h], axis=0, keepdims=True
                    )
                )
            total[eight_rows, 0:HEAD] = jnp.concatenate(reads, axis=0)
            return carry

        lax.fori_loop(0, rows // 8, eight, 0)
        read = total[:, 0:HEAD] + added
        mean = jnp.mean(read * read, axis=-1, keepdims=True)
        read = read * lax.rsqrt(mean + EPS) * head_gain[...]
        gated[h] = (read * (gate * jax.nn.sigmoid(gate))).astype(BF16)
        gather_kv(gated.at[h], (g3a, g3b)[h], (4, 15)[h], (g3a_sem, g3b_sem)[h])

    loads[n_mix].wait()
    back([(g3a, g3a_sem, 0), (g3b, g3b_sem, HEAD)], w_out, o4, p4, p4_sem, 5, m4, s4, r4, r4_sem, 6)
    add_up(nz, z_near, r4, r4_sem, total)
    own[...] = (tokens[...].astype(F32) + total[...]).astype(BF16)

    gather_tp(own, x5, 7, x5_sem)
    for copy in loads[n_mix + 1 : -1]:
        copy.wait()
    (a_at, a_size), (b_at, b_size) = ffn_chunks(up)
    parts = [
        (s6a, r6a, r6a_sem, 8, 2 * a_at, 2 * a_size),
        (s6b, r6b, r6b_sem, 9, 2 * b_at, 2 * b_size),
    ]
    projected(x5, x5_sem, 7, ffn_gain, w_ffn, parts, sq_s6, sq_r6, q6_sem, 10)

    def renew(group, carry):
        first = pl.multiple_of(group * 8, 8)
        for h in range(heads):
            at = pl.ds(h * HEAD, HEAD)
            columns = jnp.transpose(forgets[pl.ds(first, 8), at])
            value = values[pl.ds(first, 8), at]
            for b in range(8):
                v = value[b : b + 1]
                state[first + b, h] = v + columns[:, b : b + 1] * (state[first + b, h] - v)
        return carry

    lax.fori_loop(0, rows // 8, renew, 0)
    scale = factor(sq_r6, q6_sem)
    for r, landed, acc, hid, h7, h7_sem, slot in (
        (r6a, r6a_sem, acc6a, hida, h7a, h7a_sem, 11),
        (r6b, r6b_sem, acc6b, hidb, h7b, h7b_sem, 12),
    ):
        add_up(n, kv_source, r, landed, acc)
        size = hid.shape[1]
        for c in range(size // 128):
            gate = acc[:, c * 128 : (c + 1) * 128] * scale
            upper = acc[:, size + c * 128 : size + (c + 1) * 128] * scale
            hid[:, c * 128 : (c + 1) * 128] = (gate * jax.nn.sigmoid(gate) * upper).astype(BF16)
        gather_kv(hid, h7, slot, h7_sem)
    loads[-1].wait()
    gs = [(h7a, h7a_sem, a_at), (h7b, h7b_sem, b_at)]
    back(gs, w_down, o8, p8, p8_sem, 13, m8, s8, r8, r8_sem, 14)
    add_up(nz, z_near, r8, r8_sem, total)
    out[...] = (own[...].astype(F32) + total[...]).astype(BF16)

    for target, count, slot in drains:
        sent = target.at[pl.ds(0, count)]
        pltpu.make_async_copy(sent, sent, send_sem.at[slot]).wait()


def publish(rows_in, state_in, rows_out, state_out, sem):
    copies = []
    for i in range(state_in.shape[0] // 4):
        at = pl.ds(i * 4, 4)
        copies.append(pltpu.make_async_copy(state_in.at[at], state_out.at[at], sem.at[i]))
        copies[-1].start()
    rows_out[...] = rows_in[...]
    for copy in copies:
        copy.wait()


def body(
    tokens,
    state,
    mix_gain,
    q_weight,
    forget_weight,
    input_weight,
    gate_weight,
    lower_bound,
    head_gain,
    out_weight,
    ffn_gain,
    ffn_gate,
    ffn_up,
    ffn_down,
):
    n = lax.axis_size("kv")
    nx, nz = {16: (4, 8), 4: (2, 2)}[n]
    rows, cols = tokens.shape
    side, up = q_weight.shape[1], ffn_gate.shape[1]
    vmem, dma = pltpu.VMEM, pltpu.SemaphoreType.DMA
    in_vmem = pl.BlockSpec(memory_space=pltpu.VMEM)
    in_hbm = pl.BlockSpec(memory_space=pltpu.HBM)
    block = (rows, cols)
    all_blocks = vmem((n, *block), BF16)
    all_heads = vmem((n, rows, 4 * HEAD), BF16)
    chip_blocks = vmem((nz, *block), BF16)
    chip_sums = vmem((nz, *block), F32)
    squares = vmem((n, 1, 128), F32)
    (_, a_size), (_, b_size) = ffn_chunks(up)
    backward = [chip_blocks, chip_blocks, chip_sums, chip_blocks, chip_blocks]
    layer_out, new_state = pl.pallas_call(
        functools.partial(layer, n, nx, nz, cols * n),
        out_shape=(
            pltpu.VMEM(block, BF16),
            pltpu.VMEM(state.shape, F32),
        ),
        in_specs=[in_vmem, in_hbm, in_vmem, in_vmem, in_vmem, in_vmem] + [in_hbm] * 8,
        out_specs=(in_vmem, in_vmem),
        scratch_shapes=[
            vmem((cols, 4 * side), BF16),
            vmem(out_weight.shape, BF16),
            vmem((cols, 2 * up), BF16),
            vmem(ffn_down.shape, BF16),
            vmem(block, F32),
            vmem(block, F32),
            all_blocks,
            all_heads,
            all_heads,
            all_heads,
            all_heads,
            squares,
            squares,
            vmem((rows, 4 * HEAD), F32),
            vmem(block, F32),
            vmem((side // HEAD, rows, HEAD), BF16),
            vmem((n, rows, HEAD), BF16),
            vmem((n, rows, HEAD), BF16),
            *backward,
            vmem(block, BF16),
            all_blocks,
            vmem((n, rows, 2 * a_size), BF16),
            vmem((n, rows, 2 * b_size), BF16),
            vmem((n, rows, 2 * a_size), BF16),
            vmem((n, rows, 2 * b_size), BF16),
            squares,
            squares,
            vmem((rows, 2 * a_size), F32),
            vmem((rows, 2 * b_size), F32),
            vmem((rows, a_size), BF16),
            vmem((rows, b_size), BF16),
            vmem((n, rows, a_size), BF16),
            vmem((n, rows, b_size), BF16),
            *backward,
            dma((4 * (side // HEAD) + 6,)),
            dma,
            dma((16,)),
            dma((n,)),
            dma((n,)),
            dma((n,)),
            dma((n,)),
            dma((n,)),
            dma((n,)),
            dma((nz,)),
            dma((nz,)),
            dma((n,)),
            dma((n,)),
            dma((n,)),
            dma((n,)),
            dma((n,)),
            dma((n,)),
            dma((nz,)),
            dma((nz,)),
        ],
        compiler_params=pltpu.CompilerParams(
            collective_id=0, has_side_effects=True, vmem_limit_bytes=57 * 2**20
        ),
        name="layer",
    )(
        tokens,
        state,
        mix_gain.reshape(1, -1),
        lower_bound.reshape(1, -1),
        head_gain.reshape(1, -1),
        ffn_gain.reshape(1, -1),
        q_weight,
        forget_weight,
        input_weight,
        gate_weight,
        out_weight,
        ffn_gate,
        ffn_up,
        ffn_down,
    )
    return pl.pallas_call(
        publish,
        out_shape=(
            jax.ShapeDtypeStruct(block, BF16),
            jax.ShapeDtypeStruct(state.shape, F32),
        ),
        in_specs=[in_vmem, in_vmem],
        out_specs=(in_vmem, in_hbm),
        scratch_shapes=[dma((rows // 4,))],
        compiler_params=pltpu.CompilerParams(vmem_limit_bytes=8 * 2**20),
        name="publish",
    )(layer_out, new_state)


def solution(mesh):
    in_specs = (
        P("tp", "kv"),
        P("kv", "tp", None, None),
        P("kv"),
        P("kv", "tp"),
        P("kv", "tp"),
        P("kv", "tp"),
        P("kv", "tp"),
        P("tp"),
        P(),
        P("tp", "kv"),
        P("kv"),
        P("kv", "tp"),
        P("kv", "tp"),
        P("tp", "kv"),
    )
    out_specs = (P("tp", "kv"), P("kv", "tp", None, None))
    return jax.shard_map(body, mesh=mesh, in_specs=in_specs, out_specs=out_specs, check_vma=False)
```

```python
import functools

import jax
import jax.numpy as jnp
from jax import lax
from jax.experimental import pallas as pl
from jax.experimental.pallas import tpu as pltpu
from jax.sharding import PartitionSpec as P

EPS = 1e-05
MESH = pl.DeviceIdType.MESH
F32 = jnp.float32
BF16 = jnp.bfloat16
HEAD = 128


WIDE = 2 * HEAD


def layer(n, nx, nz, width, *refs):
    (
        tokens,
        state_in,
        mix_gain,
        lower_bound,
        head_gain,
        ffn_gain,
        wq_in,
        wf_in,
        wi_in,
        wg_in,
        wo_in,
        wfg_in,
        wfu_in,
        wfd_in,
        out,
        state,
        w_mix,
        w_out,
        w_ffn,
        w_down,
        forgets,
        values,
        x1,
        s2,
        t2,
        u2,
        v2,
        sq_s2,
        sq_r2,
        acc2,
        total,
        gated,
        g3a,
        g3b,
        o4,
        p4,
        m4,
        s4,
        r4,
        own,
        x5,
        s6,
        t6,
        u6,
        v6,
        d6,
        sq_s6,
        sq_r6,
        acc6,
        hida,
        hidb,
        h7a,
        h7b,
        o8,
        p8,
        m8,
        s8,
        r8,
        w_sem,
        st_sem,
        send_sem,
        x1_sem,
        t2_sem,
        v2_sem,
        q2_sem,
        g3a_sem,
        g3b_sem,
        p4_sem,
        r4_sem,
        x5_sem,
        t6_sem,
        v6_sem,
        d6_sem,
        q6_sem,
        h7a_sem,
        h7b_sem,
        p8_sem,
        r8_sem,
    ) = refs
    kv = lax.axis_index("kv")
    tp = lax.axis_index("tp")
    z, core = tp // 2, tp % 2
    mate = z * 2 + 1 - core
    ny = n // nx
    rows, cols = tokens.shape
    side = wq_in.shape[1]
    up = wfg_in.shape[1]
    heads = side // HEAD
    drains = []

    def kv_peer(j):
        x = (kv % nx + nx // 2 + nx - j % nx) % nx
        y = (kv // nx + ny // 2 + ny - j // nx) % ny
        return y * nx + x

    def kv_source(j):
        x = (kv % nx + nx // 2 + j % nx) % nx
        y = (kv // nx + ny // 2 + j // nx) % ny
        return y * nx + x

    def z_near(i):
        return (z + nz + jnp.where(i % 2 == 1, (i + 1) // 2, -(i // 2))) % nz

    def z_far(i):
        return z_near(nz - 1 - i)

    def loop(count, body):
        lax.fori_loop(0, count, lambda j, c: (body(j), c)[1], 0)

    barrier = pltpu.get_barrier_semaphore()

    def greet(who):
        pl.semaphore_signal(barrier, inc=1, device_id=who, device_id_type=MESH)

    @functools.partial(loop, n)
    def _(j):
        peer = kv_peer(j)

        @pl.when(peer != kv)
        def _():
            greet((peer, tp))

    @functools.partial(loop, nz - 1)
    def _(i):
        greet((kv, z_far(i) * 2 + core))

    greet((kv, mate))

    loads = []
    for h in range(heads):
        for k, w in enumerate((wq_in, wf_in, wi_in, wg_in)):
            loads.append(
                (w.at[:, pl.ds(h * HEAD, HEAD)], w_mix.at[:, pl.ds((4 * h + k) * HEAD, HEAD)])
            )
    n_mix = len(loads)
    loads.append((wo_in, w_out))
    units = up // HEAD
    for c in range(units):
        for k, w in enumerate((wfg_in, wfu_in)):
            loads.append(
                (w.at[:, pl.ds(c * HEAD, HEAD)], w_ffn.at[:, pl.ds((2 * c + k) * HEAD, HEAD)])
            )
    loads.append((wfd_in, w_down))
    loads = [pltpu.make_async_copy(a, b, w_sem.at[i]) for i, (a, b) in enumerate(loads)]
    for copy in loads:
        copy.start()
    state_load = pltpu.make_async_copy(state_in, state, st_sem)
    state_load.start()

    pl.semaphore_wait(barrier, (n - 1) + (nz - 1) + 1)

    def push(source, target, where, sent, landed, device):
        pltpu.make_async_remote_copy(
            src_ref=source,
            dst_ref=target.at[where],
            send_sem=sent,
            recv_sem=landed.at[where],
            device_id=device,
            device_id_type=MESH,
        ).start()

    def arrived(target, landed, who):
        pltpu.make_async_copy(target.at[who], target.at[who], landed.at[who]).wait()

    def to_kv(source, target, sent, landed, peer):
        @pl.when(peer != kv)
        def _():
            push(source, target, kv, sent, landed, (peer, tp))

        @pl.when(peer == kv)
        def _():
            pltpu.make_async_copy(source, target.at[kv], landed.at[kv]).start()

    def gather_kv(source, target, slot, landed):
        loop(n, lambda j: to_kv(source, target, send_sem.at[slot], landed, kv_peer(j)))
        drains.append((target, n - 1, slot))

    def gather_tp(source, target, slot, landed):
        target[tp] = source[...]
        sent = send_sem.at[slot]
        push(source, target, tp, sent, landed, (kv, mate))
        loop(
            nz - 1,
            lambda i: push(source, target, tp, sent, landed, (kv, z_near(i + 1) * 2 + core)),
        )
        drains.append((target, n - 1, slot))

    def projected(x, x_sem, x_slot, gain, weight, s, orders, sq_s, sq_r, q_sem, q_slot):
        ones = jnp.ones((8, cols), F32)
        lag = min(2, nz)
        sq_s[...] = jnp.zeros_like(sq_s)

        def step(i):
            @pl.when(i < nz)
            def _():
                here = z_near(i) * 2 + core

                @pl.when(i > 0)
                def _():
                    arrived(x, x_sem, here)
                    push(x.at[here], x, here, send_sem.at[x_slot], x_sem, (kv, mate))

            @pl.when(i >= lag)
            def _():
                chip = z_near(i - lag)
                arrived(x, x_sem, chip * 2 + 1 - core)
                values = x[pl.ds(chip * 2, 2)].reshape(2 * rows, cols).astype(F32)
                normed = (values * gain[...]).astype(BF16)
                for c, order in enumerate(orders):
                    product = jnp.dot(
                        normed, weight[:, c * WIDE : (c + 1) * WIDE], preferred_element_type=F32
                    ).astype(BF16)
                    for k in range(2):
                        at = chip * 2 + k
                        if order == "x":
                            at = (at % nx) * ny + at // nx
                        s[c, at] = product[k * rows : (k + 1) * rows]
                squares = lax.dot_general(
                    ones,
                    values * values,
                    (((1,), (1,)), ((), ())),
                    precision=lax.Precision.HIGHEST,
                    preferred_element_type=F32,
                )
                for k in range(2):
                    sq_s[chip * 2 + k, :, pl.ds(0, rows)] = squares[0:1, k * rows : (k + 1) * rows]

        loop(nz + lag, step)

        def send_squares():
            def send(j):
                peer = kv_peer(j)
                to_kv(sq_s.at[peer], sq_r, send_sem.at[q_slot], q_sem, peer)

            loop(n, send)
            drains.append((sq_r, n - 1, q_slot))

        return send_squares

    rings = {
        "x": (kv % nx, nx, lambda p: (kv // nx * nx + p, tp)),
        "y": (kv // nx, ny, lambda p: (p * nx + kv % nx, tp)),
    }

    def around(axis):
        me, size, _ = rings[axis]
        far_first = sorted(range(1, size), key=lambda d: -min(d, size - d))
        return [(me + d) % size for d in far_first]

    def two_stages(order, c, s, t, u, v, t_sem, v_sem, slot):
        first, second = order, "y" if order == "x" else "x"
        me, size, place = rings[first]
        then, others, then_place = rings[second]
        s, t, u, v = s.at[c], t.at[c], u.at[c], v.at[c]
        t_sem, v_sem = t_sem.at[c], v_sem.at[c]

        def start():
            for p in around(first):
                block = s.at[pl.ds(p * others, others)]
                push(block, t, me, send_sem.at[slot], t_sem, place(p))
            drains.append((t, size - 1, slot))

        def middle():
            for p in around(first):
                arrived(t, t_sem, p)
            for q in around(second) + [then]:
                sums = s[me * others + q].astype(F32)
                for p in around(first):
                    sums += t[p, q].astype(F32)
                u[q] = sums.astype(BF16)
                if q is not then:
                    push(u.at[q], v, then, send_sem.at[slot + 1], v_sem, then_place(q))
            drains.append((v, others - 1, slot + 1))

        def finish():
            for q in around(second):
                arrived(v, v_sem, q)
            sums = u[then].astype(F32)
            for q in around(second):
                sums += v[q].astype(F32)
            return sums

        return start, middle, finish

    def add_up(count, source_of, target, landed, into):
        into[...] = jnp.zeros_like(into)

        def step(j):
            who = source_of(j)
            arrived(target, landed, who)
            into[...] += target[who].astype(F32)

        loop(count, step)

    def factor(sq_r, q_sem):
        def step(j, sums):
            who = kv_source(j)
            arrived(sq_r, q_sem, who)
            return sums + sq_r[who]

        sums = lax.fori_loop(0, n, step, jnp.zeros((1, 128), F32))
        row = lax.rsqrt(sums * (1.0 / width) + EPS)
        return jnp.transpose(jnp.broadcast_to(row, (128, 128)))[0:rows]

    def back(gs, weight, o, p, p_sem, p_slot, m, s, r, r_sem, r_slot):
        def multiply(i):
            chip = z_far(i)
            pair = pl.ds(chip * 2, 2)
            product = None
            for g, landed, first in gs:
                arrived(g, landed, chip * 2)
                arrived(g, landed, chip * 2 + 1)
                size = g.shape[2]
                term = jnp.dot(
                    g[pair].reshape(2 * rows, size),
                    weight[pl.ds(first, size), :],
                    preferred_element_type=F32,
                )
                product = term if product is None else product + term
            low, high = product[0:rows], product[rows : 2 * rows]
            o[chip] = jnp.where(core == 0, high, low).astype(BF16)
            push(o.at[chip], p, chip, send_sem.at[p_slot], p_sem, (kv, mate))
            m[chip] = jnp.where(core == 0, low, high)

        def pass_on(i):
            chip = z_far(i)
            arrived(p, p_sem, chip)
            s[chip] = (m[chip] + p[chip].astype(F32)).astype(BF16)

            @pl.when(chip != z)
            def _():
                push(s.at[chip], r, z, send_sem.at[r_slot], r_sem, (kv, chip * 2 + core))

            @pl.when(chip == z)
            def _():
                pltpu.make_async_copy(s.at[chip], r.at[z], r_sem.at[z]).start()

        loop(nz, multiply)
        loop(nz, pass_on)
        drains.append((p, nz, p_slot))
        drains.append((r, nz - 1, r_slot))

    gather_tp(tokens, x1, 0, x1_sem)
    for copy in loads[0:n_mix]:
        copy.wait()
    orders = ["x", "y"] * heads
    send_squares = projected(
        x1, x1_sem, 0, mix_gain, w_mix, s2, orders, sq_s2, sq_r2, q2_sem, 1
    )
    stages = [
        two_stages(order, c, s2, t2, u2, v2, t2_sem, v2_sem, 2 + 2 * c)
        for c, order in enumerate(orders)
    ]
    for start, _, _ in stages:
        start()
    send_squares()
    for _, middle, _ in stages:
        middle()

    scale = factor(sq_r2, q2_sem)
    state_load.wait()
    for h in range(heads):
        at = pl.ds(h * HEAD, HEAD)
        acc2[:, 0:WIDE] = stages[2 * h][2]()
        acc2[:, WIDE : 2 * WIDE] = stages[2 * h + 1][2]()
        query = acc2[:, 0:HEAD] * scale
        query = query * jax.nn.sigmoid(query) * (HEAD ** (-0.5))
        low = lower_bound[:, at]
        forget = low + (1.0 - low) * jax.nn.sigmoid(acc2[:, HEAD : 2 * HEAD] * scale)
        value = acc2[:, 2 * HEAD : 3 * HEAD] * scale
        gate = acc2[:, 3 * HEAD : 4 * HEAD] * scale
        forgets[:, at] = forget
        values[:, at] = value
        kept = query * forget
        added = jnp.sum(query - kept, axis=-1, keepdims=True) * value
        acc2[:, 0:HEAD] = kept

        def eight(group, carry):
            eight_rows = pl.ds(pl.multiple_of(group * 8, 8), 8)
            columns = jnp.transpose(acc2[eight_rows, 0:HEAD])
            reads = []
            for b in range(8):
                reads.append(
                    jnp.sum(
                        columns[:, b : b + 1] * state[group * 8 + b, h], axis=0, keepdims=True
                    )
                )
            total[eight_rows, 0:HEAD] = jnp.concatenate(reads, axis=0)
            return carry

        lax.fori_loop(0, rows // 8, eight, 0)
        read = total[:, 0:HEAD] + added
        mean = jnp.mean(read * read, axis=-1, keepdims=True)
        read = read * lax.rsqrt(mean + EPS) * head_gain[...]
        gated[h] = (read * (gate * jax.nn.sigmoid(gate))).astype(BF16)
        gather_kv(gated.at[h], (g3a, g3b)[h], (10, 11)[h], (g3a_sem, g3b_sem)[h])

    loads[n_mix].wait()
    back([(g3a, g3a_sem, 0), (g3b, g3b_sem, HEAD)], w_out, o4, p4, p4_sem, 12, m4, s4, r4, r4_sem, 13)
    add_up(nz, z_near, r4, r4_sem, total)
    own[...] = (tokens[...].astype(F32) + total[...]).astype(BF16)

    gather_tp(own, x5, 14, x5_sem)
    for copy in loads[n_mix + 1 : -1]:
        copy.wait()
    orders = [("x", "y")[c % 2] for c in range(units - 1)] + ["direct"]
    send_squares = projected(
        x5, x5_sem, 14, ffn_gain, w_ffn, s6, orders, sq_s6, sq_r6, q6_sem, 15
    )
    stages = [
        two_stages(order, c, s6, t6, u6, v6, t6_sem, v6_sem, 16 + 2 * c)
        for c, order in enumerate(orders[:-1])
    ]
    for start, _, _ in stages:
        start()
    send_squares()

    def renew(group, carry):
        first = pl.multiple_of(group * 8, 8)
        for h in range(heads):
            at = pl.ds(h * HEAD, HEAD)
            columns = jnp.transpose(forgets[pl.ds(first, 8), at])
            value = values[pl.ds(first, 8), at]
            for b in range(8):
                v = value[b : b + 1]
                state[first + b, h] = v + columns[:, b : b + 1] * (state[first + b, h] - v)
        return carry

    lax.fori_loop(0, rows // 8, renew, 0)
    stages[0][1]()
    stages[1][1]()
    direct = s6.at[units - 1]
    loop(n, lambda j: to_kv(direct.at[kv_peer(j)], d6, send_sem.at[24], d6_sem, kv_peer(j)))
    drains.append((d6, n - 1, 24))
    for _, middle, _ in stages[2:]:
        middle()
    scale = factor(sq_r6, q6_sem)

    def activate(sums, hid, c):
        gate, upper = sums[:, 0:HEAD] * scale, sums[:, HEAD:WIDE] * scale
        hid[:, c * HEAD : (c + 1) * HEAD] = (gate * jax.nn.sigmoid(gate) * upper).astype(BF16)

    early = 2
    for c in range(early):
        activate(stages[c][2](), hida, c)
    gather_kv(hida, h7a, 25, h7a_sem)
    for c in range(early, units - 1):
        activate(stages[c][2](), hidb, c - early)
    add_up(n, kv_source, d6, d6_sem, acc6)
    activate(acc6[...], hidb, units - 1 - early)
    gather_kv(hidb, h7b, 26, h7b_sem)
    loads[-1].wait()
    gs = [(h7a, h7a_sem, 0), (h7b, h7b_sem, early * HEAD)]
    back(gs, w_down, o8, p8, p8_sem, 27, m8, s8, r8, r8_sem, 28)
    add_up(nz, z_near, r8, r8_sem, total)
    out[...] = (own[...].astype(F32) + total[...]).astype(BF16)

    for target, count, slot in drains:
        sent = target.at[pl.ds(0, count)]
        pltpu.make_async_copy(sent, sent, send_sem.at[slot]).wait()


def publish(rows_in, state_in, rows_out, state_out, sem):
    copies = [pltpu.make_async_copy(rows_in, rows_out, sem.at[0])]
    for i in range(state_in.shape[0] // 4):
        at = pl.ds(i * 4, 4)
        copies.append(pltpu.make_async_copy(state_in.at[at], state_out.at[at], sem.at[i + 1]))
    for copy in copies:
        copy.start()
    for copy in copies:
        copy.wait()


def body(
    tokens,
    state,
    mix_gain,
    q_weight,
    forget_weight,
    input_weight,
    gate_weight,
    lower_bound,
    head_gain,
    out_weight,
    ffn_gain,
    ffn_gate,
    ffn_up,
    ffn_down,
):
    n = lax.axis_size("kv")
    nx, nz = {16: (4, 8), 4: (2, 2)}[n]
    rows, cols = tokens.shape
    side, up = q_weight.shape[1], ffn_gate.shape[1]
    vmem, dma = pltpu.VMEM, pltpu.SemaphoreType.DMA
    in_vmem = pl.BlockSpec(memory_space=pltpu.VMEM)
    in_hbm = pl.BlockSpec(memory_space=pltpu.HBM)
    block = (rows, cols)
    all_blocks = vmem((n, *block), BF16)
    chip_blocks = vmem((nz, *block), BF16)
    chip_sums = vmem((nz, *block), F32)
    squares = vmem((n, 1, 128), F32)
    ny, wide = n // nx, 2 * HEAD
    units, mixed = up // HEAD, 2 * (side // HEAD)

    def staged(chunks):
        return [
            vmem((chunks, nx, ny, rows, wide), BF16),
            vmem((chunks, nx, rows, wide), BF16),
            vmem((chunks, nx, rows, wide), BF16),
        ]

    backward = [chip_blocks, chip_blocks, chip_sums, chip_blocks, chip_blocks]
    layer_out, new_state = pl.pallas_call(
        functools.partial(layer, n, nx, nz, cols * n),
        out_shape=(
            pltpu.VMEM(block, BF16),
            pltpu.VMEM(state.shape, F32),
        ),
        in_specs=[in_vmem, in_hbm, in_vmem, in_vmem, in_vmem, in_vmem] + [in_hbm] * 8,
        out_specs=(in_vmem, in_vmem),
        scratch_shapes=[
            vmem((cols, 4 * side), BF16),
            vmem(out_weight.shape, BF16),
            vmem((cols, 2 * up), BF16),
            vmem(ffn_down.shape, BF16),
            vmem(block, F32),
            vmem(block, F32),
            all_blocks,
            vmem((mixed, n, rows, wide), BF16),
            *staged(mixed),
            squares,
            squares,
            vmem((rows, 4 * HEAD), F32),
            vmem(block, F32),
            vmem((side // HEAD, rows, HEAD), BF16),
            vmem((n, rows, HEAD), BF16),
            vmem((n, rows, HEAD), BF16),
            *backward,
            vmem(block, BF16),
            all_blocks,
            vmem((units, n, rows, wide), BF16),
            *staged(units - 1),
            vmem((n, rows, wide), BF16),
            squares,
            squares,
            vmem((rows, wide), F32),
            vmem((rows, 2 * HEAD), BF16),
            vmem((rows, up - 2 * HEAD), BF16),
            vmem((n, rows, 2 * HEAD), BF16),
            vmem((n, rows, up - 2 * HEAD), BF16),
            *backward,
            dma((2 * mixed + 2 * units + 2,)),
            dma,
            dma((29,)),
            dma((n,)),
            dma((mixed, nx)),
            dma((mixed, nx)),
            dma((n,)),
            dma((n,)),
            dma((n,)),
            dma((nz,)),
            dma((nz,)),
            dma((n,)),
            dma((units - 1, nx)),
            dma((units - 1, nx)),
            dma((n,)),
            dma((n,)),
            dma((n,)),
            dma((n,)),
            dma((nz,)),
            dma((nz,)),
        ],
        compiler_params=pltpu.CompilerParams(
            collective_id=0, has_side_effects=True, vmem_limit_bytes=57 * 2**20
        ),
        name="layer",
    )(
        tokens,
        state,
        mix_gain.reshape(1, -1),
        lower_bound.reshape(1, -1),
        head_gain.reshape(1, -1),
        ffn_gain.reshape(1, -1),
        q_weight,
        forget_weight,
        input_weight,
        gate_weight,
        out_weight,
        ffn_gate,
        ffn_up,
        ffn_down,
    )
    return pl.pallas_call(
        publish,
        out_shape=(
            jax.ShapeDtypeStruct(block, BF16),
            jax.ShapeDtypeStruct(state.shape, F32),
        ),
        in_specs=[in_vmem, in_vmem],
        out_specs=(in_hbm, in_hbm),
        scratch_shapes=[dma((rows // 4 + 1,))],
        compiler_params=pltpu.CompilerParams(vmem_limit_bytes=8 * 2**20),
        name="publish",
    )(layer_out, new_state)


def solution(mesh):
    in_specs = (
        P("tp", "kv"),
        P("kv", "tp", None, None),
        P("kv"),
        P("kv", "tp"),
        P("kv", "tp"),
        P("kv", "tp"),
        P("kv", "tp"),
        P("tp"),
        P(),
        P("tp", "kv"),
        P("kv"),
        P("kv", "tp"),
        P("kv", "tp"),
        P("tp", "kv"),
    )
    out_specs = (P("tp", "kv"), P("kv", "tp", None, None))
    return jax.shard_map(body, mesh=mesh, in_specs=in_specs, out_specs=out_specs, check_vma=False)
```

```python
import functools

import jax
import jax.numpy as jnp
from jax import lax
from jax.experimental import pallas as pl
from jax.experimental.pallas import tpu as pltpu
from jax.sharding import PartitionSpec as P

EPS = 1e-05
MESH = pl.DeviceIdType.MESH
F32 = jnp.float32
BF16 = jnp.bfloat16
HEAD = 128


WIDE = 2 * HEAD


def layer(n, nx, nz, width, *refs):
    (
        tokens_in,
        state_in,
        mix_gain_in,
        lower_bound_in,
        head_gain_in,
        ffn_gain_in,
        wq_in,
        wf_in,
        wi_in,
        wg_in,
        wo_in,
        wfg_in,
        wfu_in,
        wfd_in,
        out,
        state_out,
        state,
        tokens,
        mix_gain,
        lower_bound,
        head_gain,
        ffn_gain,
        w_mix,
        w_out,
        w_ffn,
        w_down,
        forgets,
        values,
        x1,
        s2,
        t2,
        u2,
        v2,
        sq_s2,
        sq_r2,
        acc2,
        total,
        gated,
        g3,
        o4,
        p4,
        m4,
        s4,
        r4,
        own,
        x5,
        s6,
        t6,
        u6,
        v6,
        s7,
        t7,
        u7,
        v7,
        sq_s6,
        sq_r6,
        hidden,
        h7,
        h7c,
        o8,
        p8,
        m8,
        s8,
        r8,
        small_sem,
        w_sem,
        st_sem,
        so_sem,
        send_sem,
        x1_sem,
        t2_sem,
        v2_sem,
        q2_sem,
        g3_sem,
        p4_sem,
        r4_sem,
        x5_sem,
        t6_sem,
        v6_sem,
        t7_sem,
        v7_sem,
        q6_sem,
        h7_sem,
        h7_line_sem,
        h7c_sem,
        p8_sem,
        r8_sem,
    ) = refs
    kv = lax.axis_index("kv")
    tp = lax.axis_index("tp")
    z, core = tp // 2, tp % 2
    mate = z * 2 + 1 - core
    ny = n // nx
    rows, cols = tokens.shape
    side = wq_in.shape[1]
    up = wfg_in.shape[1]
    heads = side // HEAD
    drains = []

    def kv_peer(j):
        x = (kv % nx + nx // 2 + nx - j % nx) % nx
        y = (kv // nx + ny // 2 + ny - j // nx) % ny
        return y * nx + x

    def kv_source(j):
        x = (kv % nx + nx // 2 + j % nx) % nx
        y = (kv // nx + ny // 2 + j // nx) % ny
        return y * nx + x

    def z_near(i):
        return (z + nz + jnp.where(i % 2 == 1, (i + 1) // 2, -(i // 2))) % nz

    def z_far(i):
        return z_near(nz - 1 - i)

    def loop(count, body):
        lax.fori_loop(0, count, lambda j, c: (body(j), c)[1], 0)

    smalls = (
        (tokens_in, tokens),
        (mix_gain_in, mix_gain),
        (lower_bound_in, lower_bound),
        (head_gain_in, head_gain),
        (ffn_gain_in, ffn_gain),
    )
    smalls = [pltpu.make_async_copy(a, b, small_sem.at[i]) for i, (a, b) in enumerate(smalls)]
    for copy in smalls:
        copy.start()
    barrier = pltpu.get_barrier_semaphore()

    def greet(who):
        pl.semaphore_signal(barrier, inc=1, device_id=who, device_id_type=MESH)

    @functools.partial(loop, n)
    def _(j):
        peer = kv_peer(j)

        @pl.when(peer != kv)
        def _():
            greet((peer, tp))

    @functools.partial(loop, nz - 1)
    def _(i):
        greet((kv, z_far(i) * 2 + core))

    greet((kv, mate))

    loads = []
    for h in range(heads):
        for k, w in enumerate((wq_in, wf_in, wi_in, wg_in)):
            loads.append(
                (w.at[:, pl.ds(h * HEAD, HEAD)], w_mix.at[:, pl.ds((4 * h + k) * HEAD, HEAD)])
            )
    n_mix = len(loads)
    loads.append((wo_in, w_out))
    units = up // HEAD
    for c in range(units):
        for k, w in enumerate((wfg_in, wfu_in)):
            loads.append(
                (w.at[:, pl.ds(c * HEAD, HEAD)], w_ffn.at[:, pl.ds((2 * c + k) * HEAD, HEAD)])
            )
    loads.append((wfd_in, w_down))
    kinds = [0] * n_mix + [1] + [2] * (2 * units) + [3]
    loads = [pltpu.make_async_copy(a, b, w_sem.at[k]) for k, (a, b) in zip(kinds, loads)]
    for copy in loads:
        copy.start()
    state_load = pltpu.make_async_copy(state_in, state, st_sem)
    state_load.start()
    pl.semaphore_wait(barrier, (n - 1) + (nz - 1) + 1)
    for copy in smalls:
        copy.wait()

    def push(source, target, where, sent, landed, device):
        pltpu.make_async_remote_copy(
            src_ref=source,
            dst_ref=target.at[where],
            send_sem=sent,
            recv_sem=landed,
            device_id=device,
            device_id_type=MESH,
        ).start()

    def all_of(ref, semaphore):
        pltpu.make_async_copy(ref, ref, semaphore).wait()

    def arrived(target, landed, who):
        pltpu.make_async_copy(target.at[who], target.at[who], landed.at[who]).wait()

    def to_kv(source, target, sent, landed, peer):
        @pl.when(peer != kv)
        def _():
            push(source, target, kv, sent, landed, (peer, tp))

        @pl.when(peer == kv)
        def _():
            pltpu.make_async_copy(source, target.at[kv], landed).start()

    def gather_kv(source, target, sent, landed):
        loop(n, lambda j: to_kv(source, target, sent, landed, kv_peer(j)))

    def gather_tp(source, target, slot, landed):
        target[tp] = source[...]
        sent = send_sem.at[slot]
        push(source, target, tp, sent, landed.at[tp], (kv, mate))
        loop(
            nz - 1,
            lambda i: push(
                source, target, tp, sent, landed.at[tp], (kv, z_near(i + 1) * 2 + core)
            ),
        )
        drains.append((target.at[pl.ds(0, n - 1)], slot))

    def projected(x, x_sem, x_slot, gain, weight, s, orders, halves, sq_s, sq_r, q_sem, q_slot):
        ones = jnp.ones((8, cols), F32)
        lag = min(2, nz)
        sq_s[...] = jnp.zeros_like(sq_s)

        def step(i):
            @pl.when(i < nz)
            def _():
                here = z_near(i) * 2 + core

                @pl.when(i > 0)
                def _():
                    arrived(x, x_sem, here)
                    push(x.at[here], x, here, send_sem.at[x_slot], x_sem.at[here], (kv, mate))

            @pl.when(i >= lag)
            def _():
                chip = z_near(i - lag)
                arrived(x, x_sem, chip * 2 + 1 - core)
                values = x[pl.ds(chip * 2, 2)].reshape(2 * rows, cols).astype(F32)
                normed = (values * gain[...]).astype(BF16)
                for c, order in enumerate(orders):
                    product = jnp.dot(
                        normed, weight[:, c * WIDE : (c + 1) * WIDE], preferred_element_type=F32
                    ).astype(BF16)
                    for k in range(2):
                        y_at = chip * 2 + k
                        x_at = (y_at % nx) * ny + y_at // nx
                        part = product[k * rows : (k + 1) * rows]
                        if order == "both":
                            halves[0, x_at] = part[:, 0:HEAD]
                            halves[1, y_at] = part[:, HEAD:WIDE]
                        else:
                            s[c, x_at if order == "x" else y_at] = part
                squares = lax.dot_general(
                    ones,
                    values * values,
                    (((1,), (1,)), ((), ())),
                    precision=lax.Precision.HIGHEST,
                    preferred_element_type=F32,
                )
                for k in range(2):
                    sq_s[chip * 2 + k, :, pl.ds(0, rows)] = squares[0:1, k * rows : (k + 1) * rows]

        loop(nz + lag, step)

        def send_squares():
            def send(j):
                peer = kv_peer(j)
                to_kv(sq_s.at[peer], sq_r, send_sem.at[q_slot], q_sem, peer)

            loop(n, send)
            drains.append((sq_r.at[pl.ds(0, n - 1)], q_slot))

        return send_squares

    rings = {
        "x": (kv % nx, nx, lambda p: (kv // nx * nx + p, tp)),
        "y": (kv // nx, ny, lambda p: (p * nx + kv % nx, tp)),
    }

    def around(axis):
        me, size, _ = rings[axis]
        far_first = sorted(range(1, size), key=lambda d: -min(d, size - d))
        return [(me + d) % size for d in far_first]

    def two_stages(order, c, s, t, u, v, t_sem, v_sem, slot):
        first, second = order, "y" if order == "x" else "x"
        me, size, place = rings[first]
        then, others, then_place = rings[second]
        s, t, u, v = s.at[c], t.at[c], u.at[c], v.at[c]
        t_sem, v_sem = t_sem.at[c], v_sem.at[c]

        def start():
            for p in around(first):
                block = s.at[pl.ds(p * others, others)]
                push(block, t, me, send_sem.at[slot], t_sem, place(p))

        def middle():
            all_of(t.at[pl.ds(0, size - 1)], t_sem)
            for q in around(second) + [then]:
                sums = s[me * others + q].astype(F32)
                for p in around(first):
                    sums += t[p, q].astype(F32)
                u[q] = sums.astype(BF16)
                if q is not then:
                    push(u.at[q], v, then, send_sem.at[slot + 1], v_sem, then_place(q))

        def finish():
            all_of(v.at[pl.ds(0, others - 1)], v_sem)
            sums = u[then].astype(F32)
            for q in around(second):
                sums += v[q].astype(F32)
            return sums

        return start, middle, finish

    def spread(order, target, one_sem, two_sem, slot):
        first, second = order, "y" if order == "x" else "x"
        me, size, place = rings[first]
        then, others, then_place = rings[second]
        mine = then * size + me
        line = target.at[pl.ds(then * size, size)]

        def start():
            for p in around(first):
                push(target.at[mine], target, mine, send_sem.at[slot], one_sem, place(p))

        def forward():
            all_of(target.at[pl.ds(0, size - 1)], one_sem)
            for q in around(second):
                pltpu.make_async_remote_copy(
                    src_ref=line,
                    dst_ref=line,
                    send_sem=send_sem.at[slot + 1],
                    recv_sem=two_sem,
                    device_id=then_place(q),
                    device_id_type=MESH,
                ).start()

        def finish():
            all_of(target.at[pl.ds(0, (others - 1) * size)], two_sem)

        return mine, start, forward, finish

    def add_up(target, landed, into):
        all_of(target, landed)
        sums = target[0].astype(F32)
        for k in range(1, target.shape[0]):
            sums += target[k].astype(F32)
        into[...] = sums

    def factor(sq_r, q_sem):
        all_of(sq_r, q_sem)
        sums = jnp.zeros((1, 128), F32)
        for k in range(n):
            sums += sq_r[k]
        row = lax.rsqrt(sums * (1.0 / width) + EPS)
        return jnp.transpose(jnp.broadcast_to(row, (128, 128)))[0:rows]

    def back(gs, weight, o, p, p_sem, p_slot, m, s, r, r_sem, r_slot):
        def multiply(i):
            chip = z_far(i)
            lefts = []
            for g, order in gs:
                if order == "y":
                    at = chip * 2 % nx * ny + chip * 2 // nx
                    left = jnp.concatenate((g[at], g[at + ny]), axis=0)
                else:
                    left = g[pl.ds(chip * 2, 2)].reshape(2 * rows, g.shape[2])
                lefts.append(left)
            product = jnp.dot(
                jnp.concatenate(lefts, axis=1), weight[...], preferred_element_type=F32
            )
            low, high = product[0:rows], product[rows : 2 * rows]
            o[chip] = jnp.where(core == 0, high, low).astype(BF16)
            push(o.at[chip], p, chip, send_sem.at[p_slot], p_sem.at[chip], (kv, mate))
            m[chip] = jnp.where(core == 0, low, high)

        def pass_on(i):
            chip = z_far(i)
            arrived(p, p_sem, chip)
            s[chip] = (m[chip] + p[chip].astype(F32)).astype(BF16)

            @pl.when(chip != z)
            def _():
                push(s.at[chip], r, z, send_sem.at[r_slot], r_sem, (kv, chip * 2 + core))

            @pl.when(chip == z)
            def _():
                pltpu.make_async_copy(s.at[chip], r.at[z], r_sem).start()

        loop(nz, multiply)
        loop(nz, pass_on)
        drains.append((p, p_slot))
        drains.append((r.at[pl.ds(0, nz - 1)], r_slot))

    gather_tp(tokens, x1, 0, x1_sem)
    all_of(w_mix, w_sem.at[0])
    orders = ["x", "y"] * heads
    send_squares = projected(
        x1, x1_sem, 0, mix_gain, w_mix, s2, orders, None, sq_s2, sq_r2, q2_sem, 1
    )
    stages = [
        two_stages(order, c, s2, t2, u2, v2, t2_sem, v2_sem, 2)
        for c, order in enumerate(orders)
    ]
    send_squares()
    for start, _, _ in stages:
        start()
    for _, middle, _ in stages:
        middle()

    scale = factor(sq_r2, q2_sem)
    state_load.wait()
    for h in range(heads):
        at = pl.ds(h * HEAD, HEAD)
        acc2[:, 0:WIDE] = stages[2 * h][2]()
        acc2[:, WIDE : 2 * WIDE] = stages[2 * h + 1][2]()
        query = acc2[:, 0:HEAD] * scale
        query = query * jax.nn.sigmoid(query) * (HEAD ** (-0.5))
        low = lower_bound[:, at]
        forget = low + (1.0 - low) * jax.nn.sigmoid(acc2[:, HEAD : 2 * HEAD] * scale)
        value = acc2[:, 2 * HEAD : 3 * HEAD] * scale
        gate = acc2[:, 3 * HEAD : 4 * HEAD] * scale
        forgets[:, at] = forget
        values[:, at] = value
        kept = query * forget
        added = jnp.sum(query - kept, axis=-1, keepdims=True) * value
        for group in range(rows // 8):
            columns = jnp.transpose(kept[group * 8 : (group + 1) * 8])
            reads = []
            for b in range(8):
                reads.append(
                    jnp.sum(
                        columns[:, b : b + 1] * state[group * 8 + b, h], axis=0, keepdims=True
                    )
                )
            total[group * 8 : (group + 1) * 8, 0:HEAD] = jnp.concatenate(reads, axis=0)
        read = total[:, 0:HEAD] + added
        mean = jnp.mean(read * read, axis=-1, keepdims=True)
        read = read * lax.rsqrt(mean + EPS) * head_gain[...]
        gated[h] = (read * (gate * jax.nn.sigmoid(gate))).astype(BF16)
        gather_kv(gated.at[h], g3.at[h], send_sem.at[4], g3_sem.at[h])

    all_of(w_out, w_sem.at[1])
    for h in range(heads):
        all_of(g3.at[h], g3_sem.at[h])
    back([(g3.at[h], "x") for h in range(heads)], w_out, o4, p4, p4_sem, 5, m4, s4, r4, r4_sem, 6)
    add_up(r4, r4_sem, total)
    own[...] = (tokens[...].astype(F32) + total[...]).astype(BF16)

    gather_tp(own, x5, 7, x5_sem)
    all_of(w_ffn, w_sem.at[2])
    orders = [("x", "y")[c % 2] for c in range(units - 1)] + ["both"]
    send_squares = projected(
        x5, x5_sem, 7, ffn_gain, w_ffn, s6, orders, s7, sq_s6, sq_r6, q6_sem, 8
    )
    stages = [
        two_stages(order, c, s6, t6, u6, v6, t6_sem, v6_sem, 9)
        for c, order in enumerate(orders[:-1])
    ]
    stages += [
        two_stages("xy"[c], c, s7, t7, u7, v7, t7_sem, v7_sem, 11) for c in range(2)
    ]
    send_squares()
    for start, _, _ in stages[: units - 1]:
        start()

    def renew(group, carry):
        first = pl.multiple_of(group * 8, 8)
        for h in range(heads):
            at = pl.ds(h * HEAD, HEAD)
            columns = jnp.transpose(forgets[pl.ds(first, 8), at])
            value = values[pl.ds(first, 8), at]
            for b in range(8):
                v = value[b : b + 1]
                state[first + b, h] = v + columns[:, b : b + 1] * (state[first + b, h] - v)
        return carry

    lax.fori_loop(0, rows // 8, renew, 0)
    state_store = pltpu.make_async_copy(state, state_out, so_sem)
    state_store.start()
    stages[0][1]()
    stages[1][1]()
    for start, _, _ in stages[units - 1 :]:
        start()
    for _, middle, _ in stages[2 : units - 1]:
        middle()
    scale = factor(sq_r6, q6_sem)

    def activated(gate, upper):
        gate, upper = gate * scale, upper * scale
        return (gate * jax.nn.sigmoid(gate) * upper).astype(BF16)

    spreads = [
        spread(order, h7.at[c], h7_sem.at[c], h7_line_sem.at[c], 13)
        for c, order in enumerate(orders[:-1])
    ]

    def share(c):
        mine, start, _, _ = spreads[c]
        sums = stages[c][2]()
        h7[c, mine] = activated(sums[:, 0:HEAD], sums[:, HEAD:WIDE])
        start()

    share(0)
    share(1)
    for _, middle, _ in stages[units - 1 :]:
        middle()
    for c in range(2, units - 1):
        share(c)
    for _, _, forward, _ in spreads[:2]:
        forward()
    hidden[...] = activated(stages[units - 1][2](), stages[units][2]())
    gather_kv(hidden, h7c, send_sem.at[15], h7c_sem)
    for _, _, forward, _ in spreads[2:]:
        forward()
    for _, _, _, finish in spreads:
        finish()
    groups = [(h7.at[c], orders[c]) for c in range(units - 1)] + [(h7c, "x")]
    all_of(h7c, h7c_sem)
    all_of(w_down, w_sem.at[3])
    back(groups, w_down, o8, p8, p8_sem, 16, m8, s8, r8, r8_sem, 17)
    add_up(r8, r8_sem, total)
    out[...] = (own[...].astype(F32) + total[...]).astype(BF16)

    state_store.wait()
    last = nx - 1
    drains += [
        (t2.at[:, pl.ds(0, last)], 2),
        (v2.at[:, pl.ds(0, last)], 3),
        (g3.at[:, pl.ds(0, n - 1)], 4),
        (t6.at[:, pl.ds(0, last)], 9),
        (v6.at[:, pl.ds(0, last)], 10),
        (t7.at[:, pl.ds(0, last)], 11),
        (v7.at[:, pl.ds(0, last)], 12),
        (h7.at[:, pl.ds(0, last)], 13),
        (h7.at[:, pl.ds(0, last * nx)], 14),
        (h7c.at[pl.ds(0, n - 1)], 15),
    ]
    for sent, slot in drains:
        all_of(sent, send_sem.at[slot])


def publish(rows_in, state_in, rows_out, state_out, sem):
    copies = [pltpu.make_async_copy(rows_in, rows_out, sem.at[0])]
    for i in range(state_in.shape[0] // 4):
        at = pl.ds(i * 4, 4)
        copies.append(pltpu.make_async_copy(state_in.at[at], state_out.at[at], sem.at[i + 1]))
    for copy in copies:
        copy.start()
    for copy in copies:
        copy.wait()


def body(
    tokens,
    state,
    mix_gain,
    q_weight,
    forget_weight,
    input_weight,
    gate_weight,
    lower_bound,
    head_gain,
    out_weight,
    ffn_gain,
    ffn_gate,
    ffn_up,
    ffn_down,
):
    n = lax.axis_size("kv")
    nx, nz = {16: (4, 8), 4: (2, 2)}[n]
    rows, cols = tokens.shape
    side, up = q_weight.shape[1], ffn_gate.shape[1]
    vmem, dma = pltpu.VMEM, pltpu.SemaphoreType.DMA
    in_vmem = pl.BlockSpec(memory_space=pltpu.VMEM)
    in_hbm = pl.BlockSpec(memory_space=pltpu.HBM)
    in_place = pl.BlockSpec(memory_space=pl.ANY)
    block = (rows, cols)
    all_blocks = vmem((n, *block), BF16)
    chip_blocks = vmem((nz, *block), BF16)
    chip_sums = vmem((nz, *block), F32)
    squares = vmem((n, 1, 128), F32)
    ny, wide = n // nx, 2 * HEAD
    units, mixed = up // HEAD, 2 * (side // HEAD)

    def staged(chunks, wide=wide):
        return [
            vmem((chunks, nx, ny, rows, wide), BF16),
            vmem((chunks, nx, rows, wide), BF16),
            vmem((chunks, nx, rows, wide), BF16),
        ]

    backward = [chip_blocks, chip_blocks, chip_sums, chip_blocks, chip_blocks]
    layer_out, new_state = pl.pallas_call(
        functools.partial(layer, n, nx, nz, cols * n),
        out_shape=(
            pltpu.VMEM(block, BF16),
            pltpu.VMEM(state.shape, F32),
        ),
        in_specs=[in_hbm] * 14,
        out_specs=(in_vmem, in_place),
        scratch_shapes=[
            vmem(state.shape, F32),
            vmem(block, BF16),
            vmem((1, cols), F32),
            vmem((1, side), F32),
            vmem((1, HEAD), F32),
            vmem((1, cols), F32),
            vmem((cols, 4 * side), BF16),
            vmem(out_weight.shape, BF16),
            vmem((cols, 2 * up), BF16),
            vmem(ffn_down.shape, BF16),
            vmem(block, F32),
            vmem(block, F32),
            all_blocks,
            vmem((mixed, n, rows, wide), BF16),
            *staged(mixed),
            squares,
            squares,
            vmem((rows, 4 * HEAD), F32),
            vmem(block, F32),
            vmem((side // HEAD, rows, HEAD), BF16),
            vmem((side // HEAD, n, rows, HEAD), BF16),
            *backward,
            vmem(block, BF16),
            all_blocks,
            vmem((units - 1, n, rows, wide), BF16),
            *staged(units - 1),
            vmem((2, n, rows, HEAD), BF16),
            *staged(2, HEAD),
            squares,
            squares,
            vmem((rows, HEAD), BF16),
            vmem((units - 1, n, rows, HEAD), BF16),
            vmem((n, rows, HEAD), BF16),
            *backward,
            dma((5,)),
            dma((4,)),
            dma,
            dma,
            dma((18,)),
            dma((n,)),
            dma((mixed,)),
            dma((mixed,)),
            dma,
            dma((side // HEAD,)),
            dma((nz,)),
            dma,
            dma((n,)),
            dma((units - 1,)),
            dma((units - 1,)),
            dma((2,)),
            dma((2,)),
            dma,
            dma((units - 1,)),
            dma((units - 1,)),
            dma,
            dma((nz,)),
            dma,
        ],
        compiler_params=pltpu.CompilerParams(
            collective_id=0, has_side_effects=True, vmem_limit_bytes=57 * 2**20
        ),
        name="layer",
    )(
        tokens,
        state,
        mix_gain.reshape(1, -1),
        lower_bound.reshape(1, -1),
        head_gain.reshape(1, -1),
        ffn_gain.reshape(1, -1),
        q_weight,
        forget_weight,
        input_weight,
        gate_weight,
        out_weight,
        ffn_gate,
        ffn_up,
        ffn_down,
    )
    return pl.pallas_call(
        publish,
        out_shape=(
            jax.ShapeDtypeStruct(block, BF16),
            jax.ShapeDtypeStruct(state.shape, F32),
        ),
        in_specs=[in_place, in_place],
        out_specs=(in_hbm, in_hbm),
        scratch_shapes=[dma((rows // 4 + 1,))],
        compiler_params=pltpu.CompilerParams(vmem_limit_bytes=8 * 2**20),
        name="publish",
    )(layer_out, new_state)


def solution(mesh):
    in_specs = (
        P("tp", "kv"),
        P("kv", "tp", None, None),
        P("kv"),
        P("kv", "tp"),
        P("kv", "tp"),
        P("kv", "tp"),
        P("kv", "tp"),
        P("tp"),
        P(),
        P("tp", "kv"),
        P("kv"),
        P("kv", "tp"),
        P("kv", "tp"),
        P("tp", "kv"),
    )
    out_specs = (P("tp", "kv"), P("kv", "tp", None, None))
    return jax.shard_map(body, mesh=mesh, in_specs=in_specs, out_specs=out_specs, check_vma=False)
```

```python
import functools

import jax
import jax.numpy as jnp
from jax import lax
from jax.experimental import pallas as pl
from jax.experimental.pallas import tpu as pltpu
from jax.sharding import PartitionSpec as P

EPS = 1e-05
MESH = pl.DeviceIdType.MESH
F32 = jnp.float32
BF16 = jnp.bfloat16
HEAD = 128


WIDE = 2 * HEAD


def layer(n, nx, nz, width, *refs):
    (
        tokens_in,
        state_in,
        mix_gain_in,
        lower_bound_in,
        head_gain_in,
        ffn_gain_in,
        wq_in,
        wf_in,
        wi_in,
        wg_in,
        wo_in,
        wfg_in,
        wfu_in,
        wfd_in,
        out,
        state_out,
        state,
        tokens,
        mix_gain,
        lower_bound,
        head_gain,
        ffn_gain,
        w_mix,
        w_out,
        w_ffn,
        w_down,
        forgets,
        values,
        x1,
        s2,
        t2,
        u2,
        v2,
        sq_s2,
        sq_r2,
        total,
        gated,
        g3,
        o4,
        p4,
        m4,
        s4,
        r4,
        own,
        x5,
        s6,
        t6,
        u6,
        v6,
        s7,
        t7,
        u7,
        v7,
        sq_s6,
        sq_r6,
        hidden,
        h7,
        h7c,
        o8,
        p8,
        m8,
        s8,
        r8,
        small_sem,
        w_sem,
        st_sem,
        so_sem,
        send_sem,
        x1_sem,
        t2_sem,
        v2_sem,
        q2_sem,
        g3_sem,
        p4_sem,
        r4_sem,
        x5_sem,
        t6_sem,
        v6_sem,
        t7_sem,
        v7_sem,
        q6_sem,
        h7_sem,
        h7_line_sem,
        h7c_sem,
        p8_sem,
        r8_sem,
    ) = refs
    kv = lax.axis_index("kv")
    tp = lax.axis_index("tp")
    z, core = tp // 2, tp % 2
    mate = z * 2 + 1 - core
    ny = n // nx
    rows, cols = tokens.shape
    side = wq_in.shape[1]
    up = wfg_in.shape[1]
    heads = side // HEAD
    drains = []

    def kv_peer(j):
        x = (kv % nx + nx // 2 + nx - j % nx) % nx
        y = (kv // nx + ny // 2 + ny - j // nx) % ny
        return y * nx + x

    def kv_source(j):
        x = (kv % nx + nx // 2 + j % nx) % nx
        y = (kv // nx + ny // 2 + j // nx) % ny
        return y * nx + x

    def z_near(i):
        return (z + nz + jnp.where(i % 2 == 1, (i + 1) // 2, -(i // 2))) % nz

    def z_far(i):
        return z_near(nz - 1 - i)

    def loop(count, body):
        lax.fori_loop(0, count, lambda j, c: (body(j), c)[1], 0)

    smalls = (
        (tokens_in, tokens),
        (mix_gain_in, mix_gain),
        (lower_bound_in, lower_bound),
        (head_gain_in, head_gain),
        (ffn_gain_in, ffn_gain),
    )
    smalls = [pltpu.make_async_copy(a, b, small_sem.at[i]) for i, (a, b) in enumerate(smalls)]
    smalls[0].start()
    barrier = pltpu.get_barrier_semaphore()

    def greet(who):
        pl.semaphore_signal(barrier, inc=1, device_id=who, device_id_type=MESH)

    @functools.partial(loop, n)
    def _(j):
        peer = kv_peer(j)

        @pl.when(peer != kv)
        def _():
            greet((peer, tp))

    @functools.partial(loop, nz - 1)
    def _(i):
        greet((kv, z_far(i) * 2 + core))

    greet((kv, mate))

    loads = []
    for h in range(heads):
        for w, c in ((wq_in, 2 * h), (wf_in, 2 * h + 1), (wi_in, 2 * heads + h), (wg_in, 3 * heads + h)):
            loads.append((w.at[:, pl.ds(h * HEAD, HEAD)], w_mix.at[:, pl.ds(c * HEAD, HEAD)]))
    n_mix = len(loads)
    loads.append((wo_in, w_out))
    units = up // HEAD
    for c in range(units):
        for k, w in enumerate((wfg_in, wfu_in)):
            loads.append(
                (w.at[:, pl.ds(c * HEAD, HEAD)], w_ffn.at[:, pl.ds((2 * c + k) * HEAD, HEAD)])
            )
    loads.append((wfd_in, w_down))
    kinds = [0] * n_mix + [1] + [2] * (2 * units) + [3]
    loads = [pltpu.make_async_copy(a, b, w_sem.at[k]) for k, (a, b) in zip(kinds, loads)]
    state_load = pltpu.make_async_copy(state_in, state, st_sem)

    pl.semaphore_wait(barrier, (n - 1) + (nz - 1) + 1)
    smalls[0].wait()

    def push(source, target, where, sent, landed, device):
        pltpu.make_async_remote_copy(
            src_ref=source,
            dst_ref=target.at[where],
            send_sem=sent,
            recv_sem=landed,
            device_id=device,
            device_id_type=MESH,
        ).start()

    def all_of(ref, semaphore):
        pltpu.make_async_copy(ref, ref, semaphore).wait()

    def arrived(target, landed, who):
        pltpu.make_async_copy(target.at[who], target.at[who], landed.at[who]).wait()

    def to_kv(source, target, sent, landed, peer):
        @pl.when(peer != kv)
        def _():
            push(source, target, kv, sent, landed, (peer, tp))

        @pl.when(peer == kv)
        def _():
            pltpu.make_async_copy(source, target.at[kv], landed).start()

    def gather_kv(source, target, sent, landed):
        loop(n, lambda j: to_kv(source, target, sent, landed, kv_peer(j)))

    def gather_tp(source, target, slot, landed):
        target[tp] = source[...]
        sent = send_sem.at[slot]
        push(source, target, tp, sent, landed.at[tp], (kv, mate))
        loop(
            nz - 1,
            lambda i: push(
                source, target, tp, sent, landed.at[tp], (kv, z_near(i + 1) * 2 + core)
            ),
        )
        drains.append((target.at[pl.ds(0, n - 1)], slot))

    def projected(x, x_sem, x_slot, gain, weight, s, orders, halves, sq_s, sq_r, q_sem, q_slot):
        ones = jnp.ones((8, 2 * cols), BF16)
        lag = min(2, nz)
        sq_s[...] = jnp.zeros_like(sq_s)

        def step(i):
            @pl.when(i < nz)
            def _():
                here = z_near(i) * 2 + core

                @pl.when(i > 0)
                def _():
                    arrived(x, x_sem, here)
                    push(x.at[here], x, here, send_sem.at[x_slot], x_sem.at[here], (kv, mate))

            @pl.when(i >= lag)
            def _():
                chip = z_near(i - lag)
                arrived(x, x_sem, chip * 2 + 1 - core)
                values = x[pl.ds(chip * 2, 2)].reshape(2 * rows, cols).astype(F32)
                normed = (values * gain[...]).astype(BF16)
                for c, order in enumerate(orders):
                    product = jnp.dot(
                        normed, weight[:, c * WIDE : (c + 1) * WIDE], preferred_element_type=F32
                    ).astype(BF16)
                    for k in range(2):
                        y_at = chip * 2 + k
                        x_at = (y_at % nx) * ny + y_at // nx
                        part = product[k * rows : (k + 1) * rows]
                        if order == "both":
                            halves[0, x_at] = part[:, 0:HEAD]
                            halves[1, y_at] = part[:, HEAD:WIDE]
                        else:
                            s[c, x_at if order == "x" else y_at] = part
                squares = values * values
                high = squares.astype(BF16)
                rest = (squares - high.astype(F32)).astype(BF16)
                squares = lax.dot_general(
                    ones,
                    jnp.concatenate((high, rest), axis=1),
                    (((1,), (1,)), ((), ())),
                    preferred_element_type=F32,
                )
                for k in range(2):
                    sq_s[chip * 2 + k, :, pl.ds(0, rows)] = squares[0:1, k * rows : (k + 1) * rows]

        loop(nz + lag, step)

        def send_squares():
            def send(j):
                peer = kv_peer(j)
                to_kv(sq_s.at[peer], sq_r, send_sem.at[q_slot], q_sem, peer)

            loop(n, send)
            drains.append((sq_r.at[pl.ds(0, n - 1)], q_slot))

        return send_squares

    rings = {
        "x": (kv % nx, nx, lambda p: (kv // nx * nx + p, tp)),
        "y": (kv // nx, ny, lambda p: (p * nx + kv % nx, tp)),
    }

    def around(axis):
        me, size, _ = rings[axis]
        far_first = sorted(range(1, size), key=lambda d: -min(d, size - d))
        return [(me + d) % size for d in far_first]

    def two_stages(order, c, s, t, u, v, t_sem, v_sem, slot):
        first, second = order, "y" if order == "x" else "x"
        me, size, place = rings[first]
        then, others, then_place = rings[second]
        s, t, u, v = s.at[c], t.at[c], u.at[c], v.at[c]
        t_sem, v_sem = t_sem.at[c], v_sem.at[c]

        def start():
            for p in around(first):
                block = s.at[pl.ds(p * others, others)]
                push(block, t, me, send_sem.at[slot], t_sem, place(p))

        def middle():
            all_of(t.at[pl.ds(0, size - 1)], t_sem)
            for q in around(second) + [then]:
                sums = s[me * others + q].astype(F32)
                for p in around(first):
                    sums += t[p, q].astype(F32)
                u[q] = sums.astype(BF16)
                if q is not then:
                    push(u.at[q], v, then, send_sem.at[slot + 1], v_sem, then_place(q))

        def finish():
            all_of(v.at[pl.ds(0, others - 1)], v_sem)
            sums = u[then].astype(F32)
            for q in around(second):
                sums += v[q].astype(F32)
            return sums

        return start, middle, finish

    def spread(order, target, one_sem, two_sem, slot):
        first, second = order, "y" if order == "x" else "x"
        me, size, place = rings[first]
        then, others, then_place = rings[second]
        mine = then * size + me
        line = target.at[pl.ds(then * size, size)]

        def start():
            for p in around(first):
                push(target.at[mine], target, mine, send_sem.at[slot], one_sem, place(p))

        def forward():
            all_of(target.at[pl.ds(0, size - 1)], one_sem)
            for q in around(second):
                pltpu.make_async_remote_copy(
                    src_ref=line,
                    dst_ref=line,
                    send_sem=send_sem.at[slot + 1],
                    recv_sem=two_sem,
                    device_id=then_place(q),
                    device_id_type=MESH,
                ).start()

        def finish():
            all_of(target.at[pl.ds(0, (others - 1) * size)], two_sem)

        return mine, start, forward, finish

    def add_up(target, landed, into):
        all_of(target, landed)
        sums = target[0].astype(F32)
        for k in range(1, target.shape[0]):
            sums += target[k].astype(F32)
        into[...] = sums

    def factor(sq_r, q_sem):
        all_of(sq_r, q_sem)
        sums = jnp.zeros((1, 128), F32)
        for k in range(n):
            sums += sq_r[k]
        row = lax.rsqrt(sums * (1.0 / width) + EPS)
        return jnp.transpose(jnp.broadcast_to(row, (128, 128)))[0:rows]

    def back(gs, weight, o, p, p_sem, p_slot, m, s, r, r_sem, r_slot):
        def multiply(i):
            chip = z_far(i)
            lefts = []
            for g, order in gs:
                if order == "y":
                    at = chip * 2 % nx * ny + chip * 2 // nx
                    left = jnp.concatenate((g[at], g[at + ny]), axis=0)
                else:
                    left = g[pl.ds(chip * 2, 2)].reshape(2 * rows, g.shape[2])
                lefts.append(left)
            product = jnp.dot(
                jnp.concatenate(lefts, axis=1), weight[...], preferred_element_type=F32
            )
            low, high = product[0:rows], product[rows : 2 * rows]
            o[chip] = jnp.where(core == 0, high, low).astype(BF16)
            push(o.at[chip], p, chip, send_sem.at[p_slot], p_sem.at[chip], (kv, mate))
            m[chip] = jnp.where(core == 0, low, high)

        def pass_on(i):
            chip = z_far(i)
            arrived(p, p_sem, chip)
            s[chip] = (m[chip] + p[chip].astype(F32)).astype(BF16)

            @pl.when(chip != z)
            def _():
                push(s.at[chip], r, z, send_sem.at[r_slot], r_sem, (kv, chip * 2 + core))

            @pl.when(chip == z)
            def _():
                pltpu.make_async_copy(s.at[chip], r.at[z], r_sem).start()

        loop(nz, multiply)
        loop(nz, pass_on)
        drains.append((p, p_slot))
        drains.append((r.at[pl.ds(0, nz - 1)], r_slot))

    gather_tp(tokens, x1, 0, x1_sem)
    for copy in smalls[1:] + loads:
        copy.start()
    state_load.start()
    for copy in smalls[1:]:
        copy.wait()
    all_of(w_mix, w_sem.at[0])
    orders = ["x", "y"] * heads
    send_squares = projected(
        x1, x1_sem, 0, mix_gain, w_mix, s2, orders, None, sq_s2, sq_r2, q2_sem, 1
    )
    stages = [
        two_stages(order, c, s2, t2, u2, v2, t2_sem, v2_sem, 2)
        for c, order in enumerate(orders)
    ]
    send_squares()
    for start, _, _ in stages:
        start()
    for _, middle, _ in stages:
        middle()

    scale = factor(sq_r2, q2_sem)
    state_load.wait()
    added = []
    row_of_eight = lax.broadcasted_iota(jnp.int32, (8, HEAD), 0)
    for h in range(heads):
        at = pl.ds(h * HEAD, HEAD)
        sums = stages[h][2]()
        query = sums[:, 0:HEAD] * scale
        query = query * jax.nn.sigmoid(query) * (HEAD ** (-0.5))
        low = lower_bound[:, at]
        forget = low + (1.0 - low) * jax.nn.sigmoid(sums[:, HEAD:WIDE] * scale)
        forgets[:, at] = forget
        kept = query * forget
        added.append(jnp.sum(query - kept, axis=-1, keepdims=True))
        kept_high = kept.astype(BF16)
        kept_low = (kept - kept_high.astype(F32)).astype(BF16)
        for group in range(rows // 8):
            eight = slice(group * 8, (group + 1) * 8)
            left = jnp.concatenate(
                (kept_high[eight].astype(F32), kept_low[eight].astype(F32)), axis=0
            ).astype(BF16)
            left = jnp.concatenate((left, left), axis=1)
            reads = jnp.zeros((8, HEAD), F32)
            for b in range(8):
                right = state[group * 8 + b, h]
                high = right.astype(BF16)
                rest = (right - high.astype(F32)).astype(BF16)
                product = jnp.dot(
                    left, jnp.concatenate((high, rest), axis=0), preferred_element_type=F32
                )
                reads = jnp.where(row_of_eight == b, product[0:8] + product[8:16], reads)
            total[eight, at] = reads
    value_sums = stages[heads][2]()
    gate_sums = stages[heads + 1][2]()
    for h in range(heads):
        at = pl.ds(h * HEAD, HEAD)
        part = slice(h * HEAD, (h + 1) * HEAD)
        value = value_sums[:, part] * scale
        gate = gate_sums[:, part] * scale
        values[:, at] = value
        read = total[:, at] + added[h] * value
        mean = jnp.mean(read * read, axis=-1, keepdims=True)
        read = read * lax.rsqrt(mean + EPS) * head_gain[...]
        gated[:, at] = (read * (gate * jax.nn.sigmoid(gate))).astype(BF16)
    gather_kv(gated, g3, send_sem.at[4], g3_sem)

    all_of(w_out, w_sem.at[1])
    all_of(g3, g3_sem)
    back([(g3, "x")], w_out, o4, p4, p4_sem, 5, m4, s4, r4, r4_sem, 6)
    add_up(r4, r4_sem, total)
    own[...] = (tokens[...].astype(F32) + total[...]).astype(BF16)

    gather_tp(own, x5, 7, x5_sem)
    all_of(w_ffn, w_sem.at[2])
    orders = [("x", "y")[c % 2] for c in range(units - 1)] + ["both"]
    send_squares = projected(
        x5, x5_sem, 7, ffn_gain, w_ffn, s6, orders, s7, sq_s6, sq_r6, q6_sem, 8
    )
    stages = [
        two_stages(order, c, s6, t6, u6, v6, t6_sem, v6_sem, 9)
        for c, order in enumerate(orders[:-1])
    ]
    stages += [
        two_stages("xy"[c], c, s7, t7, u7, v7, t7_sem, v7_sem, 11) for c in range(2)
    ]
    send_squares()
    for start, _, _ in stages[: units - 1]:
        start()

    def renew(group, carry):
        first = pl.multiple_of(group * 8, 8)
        for h in range(heads):
            at = pl.ds(h * HEAD, HEAD)
            columns = jnp.transpose(forgets[pl.ds(first, 8), at])
            value = values[pl.ds(first, 8), at]
            for b in range(8):
                v = value[b : b + 1]
                state[first + b, h] = v + columns[:, b : b + 1] * (state[first + b, h] - v)
        return carry

    lax.fori_loop(0, rows // 8, renew, 0)
    state_store = pltpu.make_async_copy(state, state_out, so_sem)
    state_store.start()
    stages[0][1]()
    stages[1][1]()
    for start, _, _ in stages[units - 1 :]:
        start()
    for _, middle, _ in stages[2 : units - 1]:
        middle()
    scale = factor(sq_r6, q6_sem)

    def activated(gate, upper):
        gate, upper = gate * scale, upper * scale
        return (gate * jax.nn.sigmoid(gate) * upper).astype(BF16)

    spreads = [
        spread(order, h7.at[c], h7_sem.at[c], h7_line_sem.at[c], 13)
        for c, order in enumerate(orders[:-1])
    ]

    def share(c):
        mine, start, _, _ = spreads[c]
        sums = stages[c][2]()
        h7[c, mine] = activated(sums[:, 0:HEAD], sums[:, HEAD:WIDE])
        start()

    share(0)
    share(1)
    for _, middle, _ in stages[units - 1 :]:
        middle()
    for c in range(2, units - 1):
        share(c)
    for _, _, forward, _ in spreads[:2]:
        forward()
    hidden[...] = activated(stages[units - 1][2](), stages[units][2]())
    gather_kv(hidden, h7c, send_sem.at[15], h7c_sem)
    for _, _, forward, _ in spreads[2:]:
        forward()
    for _, _, _, finish in spreads:
        finish()
    groups = [(h7.at[c], orders[c]) for c in range(units - 1)] + [(h7c, "x")]
    all_of(h7c, h7c_sem)
    all_of(w_down, w_sem.at[3])
    back(groups, w_down, o8, p8, p8_sem, 16, m8, s8, r8, r8_sem, 17)
    add_up(r8, r8_sem, total)
    out[...] = (own[...].astype(F32) + total[...]).astype(BF16)

    state_store.wait()
    last = nx - 1
    drains += [
        (t2.at[:, pl.ds(0, last)], 2),
        (v2.at[:, pl.ds(0, last)], 3),
        (g3.at[pl.ds(0, n - 1)], 4),
        (t6.at[:, pl.ds(0, last)], 9),
        (v6.at[:, pl.ds(0, last)], 10),
        (t7.at[:, pl.ds(0, last)], 11),
        (v7.at[:, pl.ds(0, last)], 12),
        (h7.at[:, pl.ds(0, last)], 13),
        (h7.at[:, pl.ds(0, last * nx)], 14),
        (h7c.at[pl.ds(0, n - 1)], 15),
    ]
    for sent, slot in drains:
        all_of(sent, send_sem.at[slot])


def publish(rows_in, state_in, rows_out, state_out, sem):
    copies = [pltpu.make_async_copy(rows_in, rows_out, sem.at[0])]
    for i in range(state_in.shape[0] // 4):
        at = pl.ds(i * 4, 4)
        copies.append(pltpu.make_async_copy(state_in.at[at], state_out.at[at], sem.at[i + 1]))
    for copy in copies:
        copy.start()
    for copy in copies:
        copy.wait()


def body(
    tokens,
    state,
    mix_gain,
    q_weight,
    forget_weight,
    input_weight,
    gate_weight,
    lower_bound,
    head_gain,
    out_weight,
    ffn_gain,
    ffn_gate,
    ffn_up,
    ffn_down,
):
    n = lax.axis_size("kv")
    nx, nz = {16: (4, 8), 4: (2, 2)}[n]
    rows, cols = tokens.shape
    side, up = q_weight.shape[1], ffn_gate.shape[1]
    vmem, dma = pltpu.VMEM, pltpu.SemaphoreType.DMA
    in_vmem = pl.BlockSpec(memory_space=pltpu.VMEM)
    in_hbm = pl.BlockSpec(memory_space=pltpu.HBM)
    in_place = pl.BlockSpec(memory_space=pl.ANY)
    block = (rows, cols)
    all_blocks = vmem((n, *block), BF16)
    chip_blocks = vmem((nz, *block), BF16)
    chip_sums = vmem((nz, *block), F32)
    squares = vmem((n, 1, 128), F32)
    ny, wide = n // nx, 2 * HEAD
    units, mixed = up // HEAD, 2 * (side // HEAD)

    def staged(chunks, wide=wide):
        return [
            vmem((chunks, nx, ny, rows, wide), BF16),
            vmem((chunks, nx, rows, wide), BF16),
            vmem((chunks, nx, rows, wide), BF16),
        ]

    backward = [chip_blocks, chip_blocks, chip_sums, chip_blocks, chip_blocks]
    layer_out, new_state = pl.pallas_call(
        functools.partial(layer, n, nx, nz, cols * n),
        out_shape=(
            pltpu.VMEM(block, BF16),
            pltpu.VMEM(state.shape, F32),
        ),
        in_specs=[in_hbm] * 14,
        out_specs=(in_vmem, in_place),
        scratch_shapes=[
            vmem(state.shape, F32),
            vmem(block, BF16),
            vmem((1, cols), F32),
            vmem((1, side), F32),
            vmem((1, HEAD), F32),
            vmem((1, cols), F32),
            vmem((cols, 4 * side), BF16),
            vmem(out_weight.shape, BF16),
            vmem((cols, 2 * up), BF16),
            vmem(ffn_down.shape, BF16),
            vmem(block, F32),
            vmem(block, F32),
            all_blocks,
            vmem((mixed, n, rows, wide), BF16),
            *staged(mixed),
            squares,
            squares,
            vmem(block, F32),
            vmem((rows, side), BF16),
            vmem((n, rows, side), BF16),
            *backward,
            vmem(block, BF16),
            all_blocks,
            vmem((units - 1, n, rows, wide), BF16),
            *staged(units - 1),
            vmem((2, n, rows, HEAD), BF16),
            *staged(2, HEAD),
            squares,
            squares,
            vmem((rows, HEAD), BF16),
            vmem((units - 1, n, rows, HEAD), BF16),
            vmem((n, rows, HEAD), BF16),
            *backward,
            dma((5,)),
            dma((4,)),
            dma,
            dma,
            dma((18,)),
            dma((n,)),
            dma((mixed,)),
            dma((mixed,)),
            dma,
            dma,
            dma((nz,)),
            dma,
            dma((n,)),
            dma((units - 1,)),
            dma((units - 1,)),
            dma((2,)),
            dma((2,)),
            dma,
            dma((units - 1,)),
            dma((units - 1,)),
            dma,
            dma((nz,)),
            dma,
        ],
        compiler_params=pltpu.CompilerParams(
            collective_id=0, has_side_effects=True, vmem_limit_bytes=57 * 2**20
        ),
        name="layer",
    )(
        tokens,
        state,
        mix_gain.reshape(1, -1),
        lower_bound.reshape(1, -1),
        head_gain.reshape(1, -1),
        ffn_gain.reshape(1, -1),
        q_weight,
        forget_weight,
        input_weight,
        gate_weight,
        out_weight,
        ffn_gate,
        ffn_up,
        ffn_down,
    )
    return pl.pallas_call(
        publish,
        out_shape=(
            jax.ShapeDtypeStruct(block, BF16),
            jax.ShapeDtypeStruct(state.shape, F32),
        ),
        in_specs=[in_place, in_place],
        out_specs=(in_hbm, in_hbm),
        scratch_shapes=[dma((rows // 4 + 1,))],
        compiler_params=pltpu.CompilerParams(vmem_limit_bytes=8 * 2**20),
        name="publish",
    )(layer_out, new_state)


def solution(mesh):
    in_specs = (
        P("tp", "kv"),
        P("kv", "tp", None, None),
        P("kv"),
        P("kv", "tp"),
        P("kv", "tp"),
        P("kv", "tp"),
        P("kv", "tp"),
        P("tp"),
        P(),
        P("tp", "kv"),
        P("kv"),
        P("kv", "tp"),
        P("kv", "tp"),
        P("tp", "kv"),
    )
    out_specs = (P("tp", "kv"), P("kv", "tp", None, None))
    return jax.shard_map(body, mesh=mesh, in_specs=in_specs, out_specs=out_specs, check_vma=False)
```
